32 devices in a mesh: sp: 16 (over z, y, x), tp: 2 (over core).
Axes of the slice: x: 2, y: 2, z: 4, core: 2. Of those that a mesh axis runs over, the one named last changes fastest.
Arguments:
- residual: bfloat16 [2048, 4096], P('tp', 'sp'), may hold values from -6 to 6
- values: bfloat16 [4096, 4096], P('sp', 'tp'), may hold values from -6 to 6
- gate_input: bfloat16 [4096, 4096], P('sp', 'tp'), may hold values from -6 to 6
- group_keys: bfloat16 [4096, 3072], P('sp', 'tp'), may hold values from -6 to 6
- time_step: float32 [64, 4096], P('tp', 'sp'), may hold values from -8 to 14
- decay_rate: float32 [64], P('tp'), may hold values from 0 to 2
- skip_gain: float32 [64], P('tp'), may hold values from 0.25 to 2
- conv_values: bfloat16 [4, 4096], P(None, 'tp'), may hold values from -3 to 3
- conv_keys: bfloat16 [4, 3072], P(None, 'tp'), may hold values from -3 to 3
- mix_gain: float32 [4096], P('tp'), may hold values from 0.1 to 1.9
- out_weight: bfloat16 [4096, 2048], P('tp'), may hold values from -0.09375 to 0.09375
- norm_gain: float32 [2048], replicated, may hold values from 0.1 to 1.9
- hidden_gate: bfloat16 [2048, 5120], P('sp', 'tp'), may hold values from -0.125 to 0.125
- hidden_up: bfloat16 [2048, 5120], P('sp', 'tp'), may hold values from -0.125 to 0.125
- hidden_conv: bfloat16 [2, 3, 5120], P(None, None, 'tp'), may hold values from -3.5 to 3.5
- hidden_down: bfloat16 [5120, 2048], P('tp', 'sp'), may hold values from -0.078125 to 0.078125
Outputs:
- layer_out: bfloat16 [2048, 4096], P('tp', 'sp')
The draws below stay inside these ranges and needn't reach their ends.
All inputs are finite; a program needn't handle non-finite values.
Results may differ from the reference program's by a relative error of at most 0.019.
Values may be sent and summed in bfloat16 or wider, within the bound.
A program may use at most 128 MiB of HBM per device.

```python
import math
import jax
import jax.numpy as jnp
from jax import lax

D = 2048
GROUPS = 8
GROUP_HEADS = 8
HEAD_SIZE = 64
STATE_WIDE = 128
STATE_NARROW = 64
FF = 5120
BLOCK = 128
SHORT_CONV = 4
HIDDEN_CONV = 3
TOK_DEV = 256
TOKENS = 4096
HEADS = 64
INNER = 4096
KEY_COLS = 3072
N_TP = 2


def draw_time_step(key, part):
    key_span = jax.random.fold_in(key, 101)
    key_block = jax.random.fold_in(key, 102)
    key_jitter = jax.random.fold_in(key, 103)
    span_count = TOKENS // TOK_DEV
    span_rank = jnp.arange(span_count, dtype=jnp.float32).reshape(span_count, 1)
    span_trend = 2.5 * (2.0 * span_rank / (span_count - 1) - 1.0)
    span_part = span_trend + jax.random.uniform(key_span, (span_count, 1), jnp.float32, -0.6, 0.6)
    span_part = jnp.broadcast_to(span_part, (span_count, TOK_DEV)).reshape(1, TOKENS)
    block_count = TOKENS // BLOCK
    block_part = jax.random.uniform(key_block, (block_count, 1), jnp.float32, -0.3, 0.3)
    block_part = jnp.broadcast_to(block_part, (block_count, BLOCK)).reshape(1, TOKENS)
    jitter = jnp.clip(0.5 * jax.random.normal(key_jitter, (HEADS, TOKENS), jnp.float32), -1.5, 1.5)
    log_step = math.log(0.1) + span_part + block_part + jitter
    return jnp.log(jnp.expm1(jnp.exp(log_step)))


def draw_decay_rate(key, part):
    key_pick = jax.random.fold_in(key, 201)
    key_fast = jax.random.fold_in(key, 202)
    key_slow = jax.random.fold_in(key, 203)
    fast_share = 0.5
    picked = jax.random.uniform(key_pick, (HEADS,), jnp.float32) < fast_share
    fast_rate = jnp.exp(jax.random.uniform(key_fast, (HEADS,), jnp.float32, math.log(0.1), math.log(0.32)))
    slow_rate = jnp.exp(jax.random.uniform(key_slow, (HEADS,), jnp.float32, math.log(0.3), math.log(4.0))) / TOKENS
    return jnp.where(picked, fast_rate, slow_rate)


def levels(rng, shape, shards, low, largest):
    factor_of, own = 1.0, jax.random.fold_in(rng, 6)
    for position, blocks in shards:
        heights = jnp.exp(jax.random.uniform(jax.random.fold_in(own, position), (blocks,), jnp.float32, low / len(shards), largest / len(shards)))
        factor_of = factor_of * jnp.repeat(heights, shape[position] // blocks).reshape([-1 if axis == position else 1 for axis in range(len(shape))])
    return factor_of


def normal_values(rng, shape, width, reach, split=(), held_as=jnp.bfloat16):
    loudness = levels(rng, shape, split, -0.22, 0.18) if split else 1.0
    drawn = jax.random.normal(rng, shape, jnp.float32) * width * loudness
    return jnp.minimum(jnp.maximum(drawn, -reach), reach).astype(held_as)


def setup_inputs(seed: int = 0) -> dict:
    streams_of = jax.random.split(jax.random.key(seed), 17)
    residual = normal_values(streams_of[0], (D, TOKENS), 1.0, 6.0, ((0, 2), (1, 16)))
    values = normal_values(streams_of[1], (TOKENS, INNER), 1.0, 6.0, ((0, 16), (1, 2)))
    gate_input = normal_values(streams_of[2], (TOKENS, INNER), 1.0, 6.0, ((0, 16), (1, 2)))
    group_keys = normal_values(streams_of[3], (TOKENS, KEY_COLS), 1.0, 6.0, ((0, 16), (1, 2)))
    time_step = draw_time_step(jax.random.fold_in(streams_of[16], 71), 0)
    decay_rate = draw_decay_rate(jax.random.fold_in(streams_of[16], 71), 0)
    skip_gain = jnp.clip(jnp.exp(math.log(2.0) - 2.0794415 * jax.random.uniform(streams_of[6], (HEADS,), jnp.float32) ** levels(streams_of[6], (HEADS,), ((0, 2),), -0.2, 0.2)), 0.25, 2.0)
    conv_values = normal_values(streams_of[7], (SHORT_CONV, INNER), SHORT_CONV ** -0.5, 3.0, ((1, 2),))
    conv_keys = normal_values(streams_of[8], (SHORT_CONV, KEY_COLS), SHORT_CONV ** -0.5, 3.0, ((1, 2),))
    mix_gain = jnp.clip(1.0 + 0.18 * jax.random.normal(streams_of[9], (INNER,), jnp.float32), 0.1, 1.9)
    out_weight = normal_values(streams_of[10], (INNER, D), INNER ** -0.5, 0.09375, ((0, 2),))
    norm_gain = jnp.clip(1.0 + 0.18 * jax.random.normal(streams_of[11], (D,), jnp.float32), 0.1, 1.9)
    hidden_gate = normal_values(streams_of[12], (D, FF), D ** -0.5, 0.125, ((0, 16), (1, 2)))
    hidden_up = normal_values(streams_of[13], (D, FF), D ** -0.5, 0.125, ((0, 16), (1, 2)))
    hidden_conv = normal_values(streams_of[14], (2, HIDDEN_CONV, FF), HIDDEN_CONV ** -0.5, 3.5, ((2, 2),))
    hidden_down = normal_values(streams_of[15], (FF, D), FF ** -0.5, 0.078125, ((0, 2), (1, 16)))
    return dict(residual=residual, values=values, gate_input=gate_input, group_keys=group_keys, time_step=time_step, decay_rate=decay_rate, skip_gain=skip_gain, conv_values=conv_values, conv_keys=conv_keys, mix_gain=mix_gain, out_weight=out_weight, norm_gain=norm_gain, hidden_gate=hidden_gate, hidden_up=hidden_up, hidden_conv=hidden_conv, hidden_down=hidden_down)


NORM_FLOOR = 0.1
HIGHEST = lax.Precision.HIGHEST

def causal_taps(padded, weights, first_row, row_count):
    tap_count = weights.shape[0]
    window = lax.dynamic_slice_in_dim(padded, first_row, row_count + tap_count - 1, 0).astype(jnp.float32)
    summed = weights[0].astype(jnp.float32) * window[0:row_count]
    for tap_index in range(1, tap_count):
        summed = summed + weights[tap_index].astype(jnp.float32) * window[tap_index:tap_index + row_count]
    return summed

def block_heads(inputs, in_keys, out_keys, deltas, decay_rates, skip_table, carried):
    length = inputs.shape[0]
    running = jnp.cumsum(-decay_rates * deltas, axis=0)
    weighted = inputs * deltas[..., None]
    scores = jnp.einsum('ign,jgn->gij', out_keys, in_keys, precision=HIGHEST)
    by_head = jnp.transpose(running, (1, 2, 0))
    between = by_head[..., :, None] - by_head[..., None, :]
    lower_mask = jnp.tril(jnp.ones((length, length), dtype=bool))
    decays = jnp.exp(jnp.where(lower_mask, between, -jnp.inf))
    inside = jnp.einsum('ghij,jghp->ighp', scores[:, None] * decays, weighted, precision=HIGHEST)
    carried_part = jnp.einsum('ign,ghpn->ighp', out_keys, carried, precision=HIGHEST) * jnp.exp(running)[..., None]
    to_end = jnp.exp(by_head[..., -1:] - by_head)
    fresh_state = jnp.einsum('jgn,ghj,jghp->ghpn', in_keys, to_end, weighted, precision=HIGHEST)
    updated = carried * jnp.exp(by_head[..., -1])[..., None, None] + fresh_state
    return (inside + carried_part + inputs * skip_table[..., None], updated)

def sharded_sum(base, left, right, shard_count):
    share = left.shape[1] // shard_count
    summed = base
    for shard in range(shard_count):
        partial_out = jnp.dot(left[:, shard * share:(shard + 1) * share], right[shard * share:(shard + 1) * share], preferred_element_type=jnp.float32)
        partial_out = lax.optimization_barrier(partial_out.astype(jnp.bfloat16))
        summed = summed + partial_out.astype(jnp.float32)
    return summed

def reference(residual, values, gate_input, group_keys, time_step, decay_rate, skip_gain, conv_values, conv_keys, mix_gain, out_weight, norm_gain, hidden_gate, hidden_up, hidden_conv, hidden_down):
    tap_count = conv_values.shape[0]
    pad_values = jnp.pad(values, ((tap_count - 1, 0), (0, 0)))
    pad_keys = jnp.pad(group_keys, ((tap_count - 1, 0), (0, 0)))
    all_deltas = jax.nn.softplus(time_step)
    half_heads = GROUP_HEADS // 2
    wide_end = 2 * STATE_WIDE
    rate_table = decay_rate.reshape(GROUPS, GROUP_HEADS)
    skip_table = skip_gain.reshape(GROUPS, GROUP_HEADS)

    def one_block(carries, block_index):
        first_row = block_index * BLOCK
        inputs = jax.nn.silu(causal_taps(pad_values, conv_values, first_row, BLOCK)).reshape(BLOCK, GROUPS, GROUP_HEADS, HEAD_SIZE)
        key_rows = jax.nn.silu(causal_taps(pad_keys, conv_keys, first_row, BLOCK)).reshape(BLOCK, GROUPS, -1)
        deltas = lax.dynamic_slice_in_dim(all_deltas, first_row, BLOCK, 1).T.reshape(BLOCK, GROUPS, GROUP_HEADS)
        wide_out, wide_state = block_heads(inputs[:, :, :half_heads], key_rows[..., :STATE_WIDE], key_rows[..., STATE_WIDE:wide_end], deltas[:, :, :half_heads], rate_table[:, :half_heads], skip_table[:, :half_heads], carries[0])
        narrow_out, narrow_state = block_heads(inputs[:, :, half_heads:], key_rows[..., wide_end:wide_end + STATE_NARROW], key_rows[..., wide_end + STATE_NARROW:], deltas[:, :, half_heads:], rate_table[:, half_heads:], skip_table[:, half_heads:], carries[1])
        mixer_out = jnp.concatenate([wide_out, narrow_out], axis=2).reshape(BLOCK, INNER)
        gate_rows = lax.dynamic_slice_in_dim(gate_input, first_row, BLOCK, 0).astype(jnp.float32)
        gated_out = mixer_out * jax.nn.silu(gate_rows)
        inverse_rms = lax.rsqrt(lax.optimization_barrier(jnp.mean(gated_out * gated_out, axis=1, keepdims=True)) + NORM_FLOOR)
        normed = (gated_out * inverse_rms * mix_gain).astype(jnp.bfloat16)
        return ((wide_state, narrow_state), normed)
    start_state = (jnp.zeros((GROUPS, half_heads, HEAD_SIZE, STATE_WIDE), jnp.float32), jnp.zeros((GROUPS, GROUP_HEADS - half_heads, HEAD_SIZE, STATE_NARROW), jnp.float32))
    final_state, normed_blocks = lax.scan(one_block, start_state, jnp.arange(TOKENS // BLOCK, dtype=jnp.int32))
    normed_all = normed_blocks.reshape(TOKENS, INNER)
    merged = sharded_sum(residual.T.astype(jnp.float32), normed_all, out_weight, N_TP).astype(jnp.bfloat16)
    merged_wide = merged.astype(jnp.float32)
    inverse_norm = lax.rsqrt(lax.optimization_barrier(jnp.mean(merged_wide * merged_wide, axis=1, keepdims=True)) + NORM_FLOOR)
    lifted = (merged_wide * inverse_norm * norm_gain).astype(jnp.bfloat16)
    gate_pre = jnp.dot(lifted, hidden_gate, preferred_element_type=jnp.float32).astype(jnp.bfloat16)
    up_pre = jnp.dot(lifted, hidden_up, preferred_element_type=jnp.float32).astype(jnp.bfloat16)
    edge_count = hidden_conv.shape[1] - 1
    gate_conv = causal_taps(jnp.pad(gate_pre, ((edge_count, 0), (0, 0))), hidden_conv[0], 0, TOKENS)
    up_conv = causal_taps(jnp.pad(up_pre, ((edge_count, 0), (0, 0))), hidden_conv[1], 0, TOKENS)
    hidden = (jax.nn.silu(gate_conv) * up_conv).astype(jnp.bfloat16)
    layer_out = sharded_sum(merged_wide, hidden, hidden_down, N_TP).astype(jnp.bfloat16)
    return layer_out.T
```

```python
import functools

import jax
import jax.numpy as jnp
from jax import lax
from jax.experimental import pallas as pl
from jax.experimental.pallas import tpu as pltpu
from jax.sharding import PartitionSpec as P

GROUP_HEADS = 8
HEAD_SIZE = 64
STATE_WIDE = 128
STATE_NARROW = 64
BLOCK = 128


NORM_FLOOR = 0.1
SPAN = 8
EDGE = 8
TILE = 16
LANES = 128
VMEM_LIMIT = 62 * 2**20
MESH = pl.DeviceIdType.MESH
HIGHEST = lax.Precision.HIGHEST


def from_behind(value, axis, steps):
    count = lax.axis_size(axis)
    first, last = (max(0, -steps), min(count, count - steps))
    return lax.ppermute(value, axis, [(source, source + steps) for source in range(first, last)])


def earlier_states(log_spans, states, axis):
    count = lax.axis_size(axis)
    place = lax.axis_index(axis)
    slices = []
    for state in states:
        heads, size, width = state.shape
        cut = state.astype(jnp.bfloat16).reshape(heads, count, size // count * width)
        slices.append(jnp.transpose(cut, (1, 0, 2)).reshape(count, -1))
    split = slices[0].shape[1]
    high = lax.reduce_precision(log_spans, 8, 7)
    middle = lax.reduce_precision(log_spans - high, 8, 7)
    low = lax.reduce_precision(log_spans - high - middle, 8, 7)
    parts = jnp.concatenate([high, middle, low]).astype(jnp.bfloat16)
    slices.append(jnp.broadcast_to(parts, (count, parts.shape[0])))
    last = split + slices[1].shape[1]
    sent = jnp.concatenate(slices, axis=1)
    got = lax.all_to_all(sent, axis, split_axis=0, concat_axis=0, tiled=True)
    spans = got[:, last:].astype(jnp.float32).reshape(count, 3, -1).sum(axis=1)
    spot = jnp.arange(count)
    between = (spot[None, :, None] < spot) & (spot < spot[:, None, None])
    gaps = jnp.einsum("dsr,rh->dsh", between.astype(jnp.float32), spans, precision=HIGHEST)
    earlier = jnp.tril(jnp.ones((count, count), dtype=bool), -1)
    factors = jnp.exp(jnp.where(earlier[..., None], gaps, -jnp.inf))
    first = 0
    backs = []
    for state, part in zip(states, (got[:, :split], got[:, split:last])):
        heads, size, width = state.shape
        rows = part.reshape(count, heads, size // count * width)
        mine = factors[:, :, first : first + heads]
        first += heads
        backs.append(
            jnp.einsum("dsh,shn->dhn", mine.astype(jnp.bfloat16), rows, preferred_element_type=jnp.float32)
            .astype(jnp.bfloat16)
            .reshape(count, -1)
        )
    back = lax.all_to_all(
        jnp.concatenate(backs, axis=1), axis, split_axis=0, concat_axis=0, tiled=True
    )
    results = []
    for state, part in zip(states, (back[:, :split], back[:, split:])):
        heads, size, width = state.shape
        rows = part.reshape(count, heads, size // count, width)
        results.append(jnp.transpose(rows, (1, 0, 2, 3)).reshape(heads, size, width))
    return results


def from_member(shard, axis, span, turn):
    count = lax.axis_size(axis)
    return lax.ppermute(
        shard, axis, [(i, i - i % span + (i + turn) % span) for i in range(count)]
    )


def with_tp_sum(partial, rows):
    count = lax.axis_size("tp")
    place = lax.axis_index("tp")
    total = lax.dynamic_slice_in_dim(partial, place * rows, rows, 0).astype(jnp.float32)
    for turn in range(1, count):
        block = lax.dynamic_slice_in_dim(partial, (place + turn) % count * rows, rows, 0)
        total = total + from_member(block, "tp", count, turn).astype(jnp.float32)
    return total


def silu_taps(before, rows, taps):
    joined = jnp.concatenate([before.astype(jnp.float32), rows.astype(jnp.float32)], axis=0)
    count = rows.shape[0]
    first = before.shape[0] - taps.shape[0] + 1
    summed = taps[0:1].astype(jnp.float32) * joined[first : first + count]
    for tap in range(1, taps.shape[0]):
        summed = summed + taps[tap : tap + 1].astype(jnp.float32) * joined[
            first + tap : first + tap + count
        ]
    return summed * jax.nn.sigmoid(summed)


def local_heads(
    before_values, values, before_keys, keys, conv_values, conv_keys,
    run_row, run_col, delta_col, skip,
    local_out, wide_keys, narrow_keys, wide_state, narrow_state,
):
    count = values.shape[0]
    inputs = silu_taps(before_values[...], values[...], conv_values[...])
    key_rows = silu_taps(before_keys[...], keys[...], conv_keys[...]).astype(jnp.bfloat16)
    by_row, by_col, deltas = run_row[0], run_col[0], delta_col[0]
    below = lax.broadcasted_iota(jnp.int32, (count, count), 0) >= lax.broadcasted_iota(
        jnp.int32, (count, count), 1
    )
    half = GROUP_HEADS // 2
    outs = []
    for kind, (first, width, keys_out, state_out) in enumerate(
        ((0, STATE_WIDE, wide_keys, wide_state), (2 * STATE_WIDE, STATE_NARROW, narrow_keys, narrow_state))
    ):
        in_keys = key_rows[:, first : first + width]
        out_keys = key_rows[:, first + width : first + 2 * width]
        keys_out[0] = out_keys
        scores = lax.dot_general(
            out_keys, in_keys, (((1,), (1,)), ((), ())), preferred_element_type=jnp.float32
        )
        scaled = []
        for head in range(kind * half, (kind + 1) * half):
            gap = by_col[:, head : head + 1] - by_row[head : head + 1, :]
            mixing = (scores * jnp.exp(jnp.where(below, gap, -jnp.inf))).astype(jnp.bfloat16)
            own = slice(head * HEAD_SIZE, (head + 1) * HEAD_SIZE)
            weighted = inputs[:, own] * deltas[:, head : head + 1]
            outs.append(
                jnp.dot(mixing, weighted.astype(jnp.bfloat16), preferred_element_type=jnp.float32)
                + inputs[:, own] * skip[:, own]
            )
            to_end = jnp.exp(by_row[head : head + 1, count - 1 : count] - by_col[:, head : head + 1])
            scaled.append((weighted * to_end).astype(jnp.bfloat16))
        state_out[0] = lax.dot_general(
            jnp.concatenate(scaled, axis=1),
            in_keys,
            (((0,), (0,)), ((), ())),
            preferred_element_type=jnp.float32,
        ).astype(jnp.bfloat16)
    local_out[...] = jnp.concatenate(outs, axis=1)


def carried_heads(
    local_out, wide_keys, narrow_keys, wide_in, narrow_in, run_col, gates, gain, gained, squares
):
    half = GROUP_HEADS // 2
    growth = jnp.exp(run_col[0])
    parts = []
    for kind, (keys, state) in enumerate(((wide_keys, wide_in), (narrow_keys, narrow_in))):
        read = lax.dot_general(
            keys[0], state[0], (((1,), (1,)), ((), ())), preferred_element_type=jnp.float32
        )
        for spot in range(half):
            head = kind * half + spot
            parts.append(
                read[:, spot * HEAD_SIZE : (spot + 1) * HEAD_SIZE] * growth[:, head : head + 1]
            )
    gate = gates[...].astype(jnp.float32)
    gated = (local_out[...] + jnp.concatenate(parts, axis=1)) * (gate * jax.nn.sigmoid(gate))
    squares[0] = jnp.sum(gated * gated, axis=1, keepdims=True)
    gained[...] = (gated * gain[...]).astype(jnp.bfloat16)


def by_group(*shape):
    return pl.BlockSpec((1,) + shape, lambda g: (g, 0, 0))


def by_cols(rows, cols):
    return pl.BlockSpec((rows, cols), lambda g: (0, g))


def flipped(place, turn):
    result = 0
    for bit in (4, 2, 1):
        own = (place // bit) % 2
        result = result + bit * (own + (turn // bit) % 2 * (1 - 2 * own))
    return result


def row_parts(rows, count):
    bounds = [rows * part // count // TILE * TILE for part in range(count)] + [rows]
    return [slice(first, last) for first, last in zip(bounds[:-1], bounds[1:])]


def channel_mixer(
    sp_count, tp_count, span,
    merged, both_rows, down_blocks, gain, taps,
    out,
    wide, both_cols, down_rows, both_pre, edges, edge_out, edge_in, tap_wide, hidden,
    partial, tp_in, total, fold_a, fold_b, fold_c,
    own_sems, spread_send, spread_recv, side_send, side_recv, edge_send, edge_recv,
    sum_send, sum_recv, fold_send, fold_recv,
):
    rows, row_count = merged.shape
    width = both_cols.shape[0]
    quarter = width // 2
    features = both_cols.shape[1]
    sp = lax.axis_index("sp")
    tp = lax.axis_index("tp")
    place = sp % span
    base = sp - place
    own_rows = pl.ds(pl.multiple_of(tp * rows, TILE), rows)
    bits = [1 << i for i in range(span.bit_length() - 1)]
    turns = sorted(range(span), key=lambda turn: (turn.bit_count(), turn))
    slot = {turn: i for i, turn in enumerate(turns)}
    orders = [bits[i:] + bits[:i] for i in range(len(bits))]
    parts = row_parts(rows, len(bits))
    after = (sp + span) % sp_count
    behind = (sp + sp_count - span) % sp_count

    def member(turn):
        return {"sp": base + flipped(place, turn)}

    def sibling(step):
        return {"tp": (tp + step) % tp_count}

    barrier = pltpu.get_barrier_semaphore()
    greeted = [member(bit) for bit in bits] + [sibling(step) for step in range(1, tp_count)]
    if span < sp_count:
        greeted += [{"sp": after}, {"sp": behind}]
    for peer in greeted:
        pl.semaphore_signal(barrier, inc=1, device_id=peer, device_id_type=MESH)

    own_copy = pltpu.make_async_copy(merged, wide.at[0, own_rows], own_sems)
    own_copy.start()
    own_copy.wait()
    pl.semaphore_wait(barrier, len(greeted))

    def spread(part, bit, turn):
        place_rows = pl.ds(pl.multiple_of(tp * rows + parts[part].start, TILE), parts[part].stop - parts[part].start)
        index = slot[turn ^ bit] - 1
        return pltpu.make_async_remote_copy(
            src_ref=wide.at[slot[turn], place_rows],
            dst_ref=wide.at[slot[turn ^ bit], place_rows],
            send_sem=spread_send.at[part, index],
            recv_sem=spread_recv.at[part, index],
            device_id=member(bit),
            device_id_type=MESH,
        )

    def side(turn, step):
        return pltpu.make_async_remote_copy(
            src_ref=wide.at[slot[turn], own_rows],
            dst_ref=wide.at[slot[turn], own_rows],
            send_sem=side_send.at[slot[turn], step - 1],
            recv_sem=side_recv.at[slot[turn], step - 1],
            device_id=sibling(step),
            device_id_type=MESH,
        )

    started = []

    def go(copy):
        copy.start()
        started.append(copy)

    def arrived(part, turn):
        order = orders[part]
        last = [bit for bit in order if turn & bit][-1]
        spread(part, last, turn ^ last).wait_recv()

    def onward(part, turn):
        order = orders[part]
        reach = max([-1] + [i for i, bit in enumerate(order) if turn & bit])
        for bit in order[reach + 1 :]:
            go(spread(part, bit, turn))

    for position in range(len(bits)):
        for part in range(len(bits)):
            go(spread(part, orders[part][position], 0))

    def to_sides(turn):
        for step in range(1, tp_count):
            go(side(turn, step))

    def from_sides(turn):
        for step in range(1, tp_count):
            side(turn, step).wait_recv()

    to_sides(0)

    chunk = 128
    for first in range(0, features, chunk):
        cols = slice(first, first + chunk)
        block = jnp.transpose(both_rows[cols, :].astype(jnp.float32))
        both_cols[:, cols] = (block * gain[:, cols]).astype(jnp.bfloat16)
    count, _, narrow = down_blocks.shape

    @pl.loop(0, count)
    def _(index):
        block = jnp.transpose(down_blocks[index].astype(jnp.float32))
        down_rows[pl.ds(pl.multiple_of(index * narrow, narrow), narrow), :] = block.astype(jnp.bfloat16)

    for tap in range(taps.shape[1]):
        tap_wide[tap] = jnp.broadcast_to(taps[:, tap : tap + 1], (width, LANES))

    def project(index, turn):
        columns = wide[index]
        squares = jnp.zeros((8, row_count), jnp.float32)
        for first in range(0, features, 256):
            piece = columns[first : first + 256].astype(jnp.float32)
            squares = squares + jnp.sum((piece * piece).reshape(-1, 8, row_count), axis=0)
        mean = jnp.sum(squares, axis=0, keepdims=True) / features
        scale = lax.rsqrt(mean + NORM_FLOOR)
        pre = jnp.dot(both_cols[...], columns, preferred_element_type=jnp.float32) * scale
        both_pre[index] = pre.astype(jnp.bfloat16)
        edges[1 + flipped(place, turn)] = pre[:, row_count - LANES :].astype(jnp.bfloat16)

    from_sides(0)
    project(0, 0)
    events = []
    for part in range(len(bits)):
        for turn in turns[1:]:
            order = orders[part]
            key = [i for i, bit in enumerate(order) if turn & bit]
            events.append((max(key), len(key), key, part, turn))
    waiting = {turn: len(bits) for turn in turns[1:]}
    pending = []
    for _, _, _, part, turn in sorted(events):
        arrived(part, turn)
        onward(part, turn)
        waiting[turn] -= 1
        if waiting[turn] == 0:
            to_sides(turn)
            pending.append(turn)
            if len(pending) > 1:
                done = pending.pop(0)
                from_sides(done)
                project(slot[done], done)
    for done in pending:
        from_sides(done)
        project(slot[done], done)

    if span < sp_count:
        last = jnp.transpose(edges[span].astype(jnp.float32))
        edge_out[...] = last[LANES - TILE :, :].astype(jnp.bfloat16)
        edge_copy = pltpu.make_async_remote_copy(
            src_ref=edge_out, dst_ref=edge_in, send_sem=edge_send, recv_sem=edge_recv,
            device_id={"sp": after}, device_id_type=MESH,
        )
        edge_copy.start()
    edges[0] = jnp.zeros(edges.shape[1:], edges.dtype)

    lane = lax.broadcasted_iota(jnp.int32, (quarter, LANES), 1)

    def taps_of(index, spot):
        for first in range(0, row_count, LANES):
            sums = []
            for kind in range(2):
                own = slice(kind * quarter, (kind + 1) * quarter)
                now = both_pre[index, own, first : first + LANES].astype(jnp.float32)
                if first:
                    past = both_pre[index, own, first - LANES : first].astype(jnp.float32)
                else:
                    past = edges[spot, own, :].astype(jnp.float32)
                tap_count = taps.shape[1]
                summed = tap_wide[tap_count - 1, own, :] * now
                for back in range(1, tap_count):
                    moved = jnp.where(lane < back, pltpu.roll(past, back, 1), pltpu.roll(now, back, 1))
                    summed = summed + tap_wide[tap_count - 1 - back, own, :] * moved
                sums.append(summed)
            value = sums[0] * jax.nn.sigmoid(sums[0]) * sums[1]
            hidden[index, :, first : first + LANES] = value.astype(jnp.bfloat16)

    for turn in turns:
        taps_of(slot[turn], flipped(place, turn))
    if span < sp_count:
        edge_copy.wait()
        last = jnp.transpose(edge_in[...].astype(jnp.float32))
        own_edge = jnp.where(base == 0, 0.0, last)
        edges[0, :, LANES - TILE :] = own_edge.astype(jnp.bfloat16)
        for turn in turns:
            @pl.when(flipped(place, turn) == 0)
            def _():
                taps_of(slot[turn], 0)

    def to_sum(turn, step):
        peer = pl.ds(pl.multiple_of((tp + step) % tp_count * rows, TILE), rows)
        return pltpu.make_async_remote_copy(
            src_ref=partial.at[slot[turn], peer],
            dst_ref=tp_in.at[slot[turn], step - 1],
            send_sem=sum_send.at[slot[turn], step - 1],
            recv_sem=sum_recv.at[slot[turn], step - 1],
            device_id=sibling(step),
            device_id_type=MESH,
        )

    folds = (fold_a, fold_b, fold_c)

    def fold(part, stage, turn):
        bit = orders[part][stage]
        here = slot[turn ^ bit]
        return pltpu.make_async_remote_copy(
            src_ref=total.at[slot[turn], parts[part]],
            dst_ref=folds[stage].at[here, parts[part]],
            send_sem=fold_send.at[part, slot[turn] - 1],
            recv_sem=fold_recv.at[part, stage, here],
            device_id=member(bit),
            device_id_type=MESH,
        )

    def stage_of(part, turn):
        return min(i for i, bit in enumerate(orders[part]) if turn & bit)

    def multiply(turn):
        step_rows = min(512, features)
        for first in range(0, features, step_rows):
            block = slice(first, first + step_rows)
            partial[slot[turn], block] = jnp.dot(
                down_rows[block, :], hidden[slot[turn]], preferred_element_type=jnp.float32
            ).astype(jnp.bfloat16)
        for step in range(1, tp_count):
            go(to_sum(turn, step))

    def add_up(turn):
        summed = partial[slot[turn], own_rows].astype(jnp.float32)
        for step in range(1, tp_count):
            to_sum(turn, step).wait_recv()
            summed = summed + tp_in[slot[turn], step - 1].astype(jnp.float32)
        total[slot[turn]] = summed.astype(jnp.bfloat16)
        if turn:
            for part in range(len(bits)):
                if stage_of(part, turn) == 0:
                    go(fold(part, 0, turn))

    line = turns[::-1]
    for position, turn in enumerate(line):
        multiply(turn)
        if position:
            add_up(line[position - 1])
    add_up(line[-1])
    for stage in range(len(bits)):
        for part in range(len(bits)):
            order = orders[part]
            left = [turn for turn in turns if not any(turn & bit for bit in order[: stage + 1])]
            for turn in sorted(left, key=lambda turn: -turn.bit_count()):
                fold(part, stage, turn ^ order[stage]).wait_recv()
                summed = total[slot[turn], parts[part]].astype(jnp.float32) + folds[stage][
                    slot[turn], parts[part]
                ].astype(jnp.float32)
                if turn:
                    total[slot[turn], parts[part]] = summed.astype(jnp.bfloat16)
                    if stage_of(part, turn) == stage + 1:
                        go(fold(part, stage + 1, turn))
                elif stage + 1 < len(bits):
                    total[0, parts[part]] = summed.astype(jnp.bfloat16)
                else:
                    out[parts[part], :] = (merged[parts[part], :].astype(jnp.float32) + summed).astype(jnp.bfloat16)
    for copy in started:
        copy.wait_send()


def mixed_channels(merged, both_rows, down_blocks, gain, taps, span):
    rows, row_count = merged.shape
    sp_count, tp_count = lax.axis_size("sp"), lax.axis_size("tp")
    features, width = both_rows.shape
    quarter = width // 2
    levels = span.bit_length() - 1
    bf = jnp.bfloat16
    dma = pltpu.SemaphoreType.DMA
    vmem = pl.BlockSpec(memory_space=pltpu.VMEM)
    return pl.pallas_call(
        functools.partial(channel_mixer, sp_count, tp_count, span),
        in_specs=[vmem] * 5,
        out_specs=vmem,
        out_shape=jax.ShapeDtypeStruct((rows, row_count), bf),
        scratch_shapes=[
            pltpu.VMEM((span, features, row_count), bf),
            pltpu.VMEM((width, features), bf),
            pltpu.VMEM((features, quarter), bf),
            pltpu.VMEM((span, width, row_count), bf),
            pltpu.VMEM((span + 1, width, LANES), bf),
            pltpu.VMEM((TILE, width), bf),
            pltpu.VMEM((TILE, width), bf),
            pltpu.VMEM((taps.shape[1], width, LANES), jnp.float32),
            pltpu.VMEM((span, quarter, row_count), bf),
            pltpu.VMEM((span, features, row_count), bf),
            pltpu.VMEM((span, tp_count - 1, rows, row_count), bf),
            pltpu.VMEM((span, rows, row_count), bf),
            pltpu.VMEM((span, rows, row_count), bf),
            pltpu.VMEM((4, rows, row_count), bf),
            pltpu.VMEM((1, rows, row_count), bf),
            dma,
            dma((levels, span - 1)),
            dma((levels, span - 1)),
            dma((span, tp_count - 1)),
            dma((span, tp_count - 1)),
            dma,
            dma,
            dma((span, tp_count - 1)),
            dma((span, tp_count - 1)),
            dma((levels, span - 1)),
            dma((levels, levels, span)),
        ],
        compiler_params=pltpu.CompilerParams(
            collective_id=1, has_side_effects=True, vmem_limit_bytes=VMEM_LIMIT
        ),
        cost_estimate=pl.CostEstimate(flops=10**11, bytes_accessed=10**7, transcendentals=10**6),
        name="channel_mixer",
    )(merged, both_rows, down_blocks, gain, taps)


def hidden_weights(hidden_gate, hidden_up, hidden_down, span):
    count = lax.axis_size("sp")
    rows, hidden_cols = hidden_gate.shape
    quarter = hidden_cols // span
    gates = hidden_gate.reshape(rows, span, quarter)
    ups = hidden_up.reshape(rows, span, quarter)
    both = jnp.transpose(jnp.concatenate([gates, ups], axis=2), (1, 0, 2))
    down = hidden_down.reshape(span, quarter, hidden_down.shape[1])
    both = jnp.concatenate([both] * (count // span), axis=0)
    down = jnp.concatenate([down] * (count // span), axis=0)
    both = lax.all_to_all(both, "sp", 0, 0, tiled=True)
    both, down = lax.optimization_barrier((both, down))
    down = lax.all_to_all(down, "sp", 0, 0, tiled=True)
    return both.reshape(count * rows, 2 * quarter), down


def local(
    residual,
    values,
    gate_input,
    group_keys,
    time_step,
    decay_rate,
    skip_gain,
    conv_values,
    conv_keys,
    mix_gain,
    out_weight,
    norm_gain,
    hidden_gate,
    hidden_up,
    hidden_conv,
    hidden_down,
):
    row_count = values.shape[0]
    value_cols = values.shape[1]
    tap_count = conv_values.shape[0]
    sp_count = lax.axis_size("sp")
    span = min(SPAN, sp_count)
    member = lax.axis_index("sp") % span
    both_rows, down_blocks = hidden_weights(hidden_gate, hidden_up, hidden_down, span)
    quarter = down_blocks.shape[1]
    tail_rows = jnp.concatenate([values[row_count - EDGE :], group_keys[row_count - EDGE :]], axis=1)
    before_rows = from_behind(tail_rows, "sp", 1)
    group_keys_cols = 2 * STATE_WIDE + 2 * STATE_NARROW
    group_count = group_keys.shape[1] // group_keys_cols
    group_cols = GROUP_HEADS * HEAD_SIZE
    half_rows = group_cols // 2
    deltas = jax.nn.softplus(time_step)
    running = jnp.cumsum(-decay_rate[:, None] * deltas, axis=1)
    run_row = running.reshape(group_count, GROUP_HEADS, row_count)
    run_col = jnp.transpose(run_row, (0, 2, 1))
    delta_col = jnp.transpose(deltas.reshape(group_count, GROUP_HEADS, row_count), (0, 2, 1))
    skip = jnp.repeat(skip_gain, HEAD_SIZE)[None, :]
    local_out, wide_keys, narrow_keys, wide_state, narrow_state = pl.pallas_call(
        local_heads,
        grid=(group_count,),
        in_specs=[
            by_cols(EDGE, group_cols),
            by_cols(row_count, group_cols),
            by_cols(EDGE, group_keys_cols),
            by_cols(row_count, group_keys_cols),
            by_cols(tap_count, group_cols),
            by_cols(tap_count, group_keys_cols),
            by_group(GROUP_HEADS, row_count),
            by_group(row_count, GROUP_HEADS),
            by_group(row_count, GROUP_HEADS),
            by_cols(1, group_cols),
        ],
        out_specs=[
            by_cols(row_count, group_cols),
            by_group(row_count, STATE_WIDE),
            by_group(row_count, STATE_NARROW),
            by_group(half_rows, STATE_WIDE),
            by_group(half_rows, STATE_NARROW),
        ],
        out_shape=[
            jax.ShapeDtypeStruct((row_count, value_cols), jnp.float32),
            jax.ShapeDtypeStruct((group_count, row_count, STATE_WIDE), jnp.bfloat16),
            jax.ShapeDtypeStruct((group_count, row_count, STATE_NARROW), jnp.bfloat16),
            jax.ShapeDtypeStruct((group_count, half_rows, STATE_WIDE), jnp.bfloat16),
            jax.ShapeDtypeStruct((group_count, half_rows, STATE_NARROW), jnp.bfloat16),
        ],
        cost_estimate=pl.CostEstimate(flops=10**9, bytes_accessed=10**7, transcendentals=10**6),
        name="local_heads",
    )(
        before_rows[:, :value_cols],
        values,
        before_rows[:, value_cols:],
        group_keys,
        conv_values,
        conv_keys,
        run_row,
        run_col,
        delta_col,
        skip,
    )
    spans = run_row[:, :, -1]
    half_heads = GROUP_HEADS // 2
    incoming = earlier_states(
        jnp.concatenate(
            [spans[:, :half_heads].reshape(-1), spans[:, half_heads:].reshape(-1)]
        ),
        (
            wide_state.reshape(-1, HEAD_SIZE, STATE_WIDE),
            narrow_state.reshape(-1, HEAD_SIZE, STATE_NARROW),
        ),
        "sp",
    )
    gained, squares = pl.pallas_call(
        carried_heads,
        grid=(group_count,),
        in_specs=[
            by_cols(row_count, group_cols),
            by_group(row_count, STATE_WIDE),
            by_group(row_count, STATE_NARROW),
            by_group(half_rows, STATE_WIDE),
            by_group(half_rows, STATE_NARROW),
            by_group(row_count, GROUP_HEADS),
            by_cols(row_count, group_cols),
            by_cols(1, group_cols),
        ],
        out_specs=[by_cols(row_count, group_cols), by_group(row_count, 1)],
        out_shape=[
            jax.ShapeDtypeStruct((row_count, value_cols), jnp.bfloat16),
            jax.ShapeDtypeStruct((group_count, row_count, 1), jnp.float32),
        ],
        cost_estimate=pl.CostEstimate(flops=10**8, bytes_accessed=10**7, transcendentals=10**6),
        name="carried_heads",
    )(
        local_out,
        wide_keys,
        narrow_keys,
        incoming[0].reshape(wide_state.shape),
        incoming[1].reshape(narrow_state.shape),
        run_col,
        gate_input,
        mix_gain[None, :],
    )
    squares = lax.psum(jnp.sum(squares[:, :, 0], axis=0), "tp")
    inverse_rms = lax.rsqrt(squares / (value_cols * lax.axis_size("tp")) + NORM_FLOOR)
    mixer_part = lax.dot_general(
        out_weight, gained, (((0,), (1,)), ((), ())), preferred_element_type=jnp.float32
    ).astype(jnp.bfloat16)
    own_rows = residual.shape[0]
    mixer_sum = with_tp_sum(mixer_part, own_rows) * inverse_rms[None, :]
    own_merged = (residual.astype(jnp.float32) + mixer_sum).astype(jnp.bfloat16)
    own_taps = lax.dynamic_slice_in_dim(hidden_conv, member * quarter, quarter, 2)
    own_taps = jnp.transpose(own_taps, (0, 2, 1)).reshape(2 * quarter, -1).astype(jnp.float32)
    return mixed_channels(own_merged, both_rows, down_blocks, norm_gain[None, :], own_taps, span)


def solution(mesh):
    in_specs = (
        P("tp", "sp"),
        P("sp", "tp"),
        P("sp", "tp"),
        P("sp", "tp"),
        P("tp", "sp"),
        P("tp"),
        P("tp"),
        P(None, "tp"),
        P(None, "tp"),
        P("tp"),
        P("tp", None),
        P(),
        P("sp", "tp"),
        P("sp", "tp"),
        P(None, None, "tp"),
        P("tp", "sp"),
    )
    out_specs = P("tp", "sp")
    return jax.shard_map(local, mesh=mesh, in_specs=in_specs, out_specs=out_specs, check_vma=False)
```

```python
import functools

import jax
import jax.numpy as jnp
from jax import lax
from jax.experimental import pallas as pl
from jax.experimental.pallas import tpu as pltpu
from jax.sharding import PartitionSpec as P

GROUP_HEADS = 8
HEAD_SIZE = 64
STATE_WIDE = 128
STATE_NARROW = 64

NORM_FLOOR = 0.1
SPAN = 8
EDGE = 8
TILE = 16
LANES = 128
FIRST_BLOCKS = 1
SECOND_BLOCKS = 1
VMEM_LIMIT = 62 * 2**20
MESH = pl.DeviceIdType.MESH
HIGHEST = lax.Precision.HIGHEST


def flipped(place, turn, count):
    result = 0
    bit = 1
    while bit < count:
        own = (place // bit) % 2
        result = result + bit * (own + (turn // bit) % 2 * (1 - 2 * own))
        bit *= 2
    return result


def silu_taps(before, rows, taps):
    joined = jnp.concatenate([before.astype(jnp.float32), rows.astype(jnp.float32)], axis=0)
    count = rows.shape[0]
    first = before.shape[0] - taps.shape[0] + 1
    summed = taps[0:1].astype(jnp.float32) * joined[first : first + count]
    for tap in range(1, taps.shape[0]):
        summed = summed + taps[tap : tap + 1].astype(jnp.float32) * joined[
            first + tap : first + tap + count
        ]
    return summed * jax.nn.sigmoid(summed)


def causal_rows(value, count):
    row = lax.broadcasted_iota(jnp.int32, (count, count), 0)
    col = lax.broadcasted_iota(jnp.int32, (count, count), 1)
    return jnp.where(row >= col, value, -jnp.inf)


def token_mixer(
    sp_count, tp_count, span,
    values, keys, gates_far, time_step, decay_rate, skip, conv_values, conv_keys, mix_gain,
    weight_far, residual, both_far,
    merged, both_got,
    gates, weight, values_tail, keys_tail, run, delta, inputs, key_rows, local_out, gained,
    state, state_got, states_out, states_in, ends_own, ends, squares_own, squares_in,
    partial, partial_in,
    local_sems, tail_send, tail_recv, ends_send, ends_recv, state_send, state_recv,
    back_send, back_recv, square_send, square_recv, sum_send, sum_recv, both_send, both_recv,
):
    row_count = values.shape[0]
    head_count = time_step.shape[0]
    groups = head_count // GROUP_HEADS
    half = GROUP_HEADS // 2
    key_cols = 2 * STATE_WIDE + 2 * STATE_NARROW
    group_cols = GROUP_HEADS * HEAD_SIZE
    wide_rows = half * HEAD_SIZE
    narrow_rows = wide_rows * STATE_NARROW // STATE_WIDE
    group_rows = wide_rows + narrow_rows
    slice_rows = states_out.shape[1]
    owners = groups * group_rows // slice_rows
    rows = residual.shape[0]
    features = weight.shape[1]
    sp = lax.axis_index("sp")
    tp = lax.axis_index("tp")

    gate_copy = pltpu.make_async_copy(gates_far, gates, local_sems.at[0])
    gate_copy.start()
    weight_copy = pltpu.make_async_copy(weight_far, weight, local_sems.at[1])
    weight_copy.start()
    both_copy = pltpu.make_async_copy(both_far.at[sp % span], both_got.at[sp], local_sems.at[2])
    both_copy.start()

    others = [{"sp": flipped(sp, turn, sp_count)} for turn in range(1, sp_count)]
    siblings = [{"tp": (tp + step) % tp_count} for step in range(1, tp_count)]
    barrier = pltpu.get_barrier_semaphore()
    for peer in others + siblings:
        pl.semaphore_signal(barrier, inc=1, device_id=peer, device_id_type=MESH)

    deltas = jnp.maximum(time_step[...], 0.0) + jnp.log1p(jnp.exp(-jnp.abs(time_step[...])))
    delta[...] = deltas
    upto = lax.broadcasted_iota(jnp.int32, (row_count, row_count), 0) <= lax.broadcasted_iota(
        jnp.int32, (row_count, row_count), 1
    )
    running = jnp.dot(
        -decay_rate[...] * deltas, upto.astype(jnp.float32),
        precision=HIGHEST, preferred_element_type=jnp.float32,
    )
    run[...] = running
    tail_heads = jnp.concatenate(
        [running[:, row_count - LANES :], jnp.zeros((LANES - head_count, LANES), jnp.float32)], axis=0
    )
    last_rows = jnp.transpose(tail_heads)[LANES - 8 :, :]
    ends_own[...] = last_rows
    ends[sp] = last_rows

    pl.semaphore_wait(barrier, len(others) + len(siblings))

    started = []

    def go(copy):
        copy.start()
        started.append(copy)

    def remote(source, target, send, recv, peer):
        return pltpu.make_async_remote_copy(
            src_ref=source, dst_ref=target, send_sem=send, recv_sem=recv,
            device_id=peer, device_id_type=MESH,
        )

    after = {"sp": (sp + 1) % sp_count}
    last = slice(row_count - TILE, row_count)
    tails = [
        remote(values.at[last], values_tail, tail_send.at[0], tail_recv.at[0], after),
        remote(keys.at[last], keys_tail, tail_send.at[1], tail_recv.at[1], after),
    ]
    for copy in tails:
        go(copy)

    def both_block(turn):
        peer = flipped(sp, turn, sp_count)
        return remote(
            both_far.at[peer % span], both_got.at[sp], both_send.at[turn - 1], both_recv.at[turn - 1],
            {"sp": peer},
        )

    queue = list(range(sp_count - 1, 0, -1))

    def feed(count):
        for turn in queue[:count]:
            go(both_block(turn))
        del queue[:count]

    for turn in range(1, sp_count):
        peer = {"sp": flipped(sp, turn, sp_count)}
        go(remote(ends_own, ends.at[sp], ends_send.at[turn - 1], ends_recv.at[turn - 1], peer))
    feed(FIRST_BLOCKS)
    for copy in tails:
        copy.wait_recv()

    def heads_of(g):
        spot = pl.ds(pl.multiple_of(g * GROUP_HEADS, GROUP_HEADS), GROUP_HEADS)
        by_row = run[spot, :]
        return by_row, jnp.transpose(by_row), jnp.transpose(delta[spot, :])

    def value_cols(g):
        return pl.ds(pl.multiple_of(g * group_cols, LANES), group_cols)

    def keys_at(g, first, width):
        return key_rows[g, :, first : first + width]

    kinds = ((0, STATE_WIDE), (2 * STATE_WIDE, STATE_NARROW))

    def state_copy(owner, own_slice):
        return remote(
            state.at[own_slice], state_got.at[sp], state_send.at[owner], state_recv.at[sp], {"sp": owner}
        )

    def rows_of(owner):
        return pl.ds(pl.multiple_of(owner * slice_rows, 8), slice_rows)

    @pl.loop(0, groups)
    def _(g):
        cols = value_cols(g)
        key_span = pl.ds(pl.multiple_of(g * key_cols, LANES), key_cols)
        first = sp == 0
        before = jnp.where(first, 0.0, values_tail[TILE - 8 :, cols].astype(jnp.float32))
        inner = silu_taps(before, values[:, cols], conv_values[:, cols])
        inputs[:, cols] = inner
        before = jnp.where(first, 0.0, keys_tail[TILE - 8 :, key_span].astype(jnp.float32))
        made = silu_taps(before, keys[:, key_span], conv_keys[:, key_span]).astype(jnp.bfloat16)
        key_rows[g] = made
        by_row, by_col, deltas = heads_of(g)
        states = []
        for kind, (first_col, width) in enumerate(kinds):
            scaled = []
            for head in range(kind * half, (kind + 1) * half):
                own = slice(head * HEAD_SIZE, (head + 1) * HEAD_SIZE)
                to_end = jnp.exp(by_row[head : head + 1, row_count - 1 :] - by_col[:, head : head + 1])
                scaled.append((inner[:, own] * (deltas[:, head : head + 1] * to_end)).astype(jnp.bfloat16))
            states.append(
                lax.dot_general(
                    jnp.concatenate(scaled, axis=1),
                    made[:, first_col : first_col + width],
                    (((0,), (0,)), ((), ())),
                    preferred_element_type=jnp.float32,
                ).astype(jnp.bfloat16)
            )
        base = pl.multiple_of(g * group_rows, 8)
        state[pl.ds(base, wide_rows), :] = states[0]
        fold = STATE_WIDE // STATE_NARROW
        state[pl.ds(base + wide_rows, narrow_rows), :] = jnp.concatenate(
            [states[1][i * narrow_rows : (i + 1) * narrow_rows] for i in range(fold)], axis=1
        )
        per_group = group_rows // slice_rows

        @pl.loop(0, per_group)
        def _(index):
            owner = g * per_group + index

            @pl.when(owner != sp)
            def _():
                state_copy(owner, rows_of(owner)).start()

    feed(SECOND_BLOCKS)

    def inside(g):
        cols = value_cols(g)
        by_row, by_col, deltas = heads_of(g)
        inner = inputs[:, cols]
        outs = []
        for kind, (first_col, width) in enumerate(kinds):
            scores = lax.dot_general(
                keys_at(g, first_col + width, width), keys_at(g, first_col, width),
                (((1,), (1,)), ((), ())), preferred_element_type=jnp.float32,
            )
            for head in range(kind * half, (kind + 1) * half):
                own = slice(head * HEAD_SIZE, (head + 1) * HEAD_SIZE)
                gap = causal_rows(by_col[:, head : head + 1] - by_row[head : head + 1, :], row_count)
                mixing = (scores * jnp.exp(gap)).astype(jnp.bfloat16)
                weighted = (inner[:, own] * deltas[:, head : head + 1]).astype(jnp.bfloat16)
                outs.append(jnp.dot(mixing, weighted, preferred_element_type=jnp.float32))
        local_out[:, cols] = jnp.concatenate(outs, axis=1) + inner * skip[:, cols]

    ahead = (groups + 1) // 2
    @pl.loop(0, ahead)
    def _(g):
        inside(g)

    for turn in range(1, sp_count):
        peer = {"sp": flipped(sp, turn, sp_count)}
        remote(ends_own, ends.at[sp], ends_send.at[turn - 1], ends_recv.at[turn - 1], peer).wait_recv()

    def carry_all():
        for turn in range(1, sp_count):
            source = flipped(sp, turn, sp_count)
            remote(
                state.at[rows_of(sp)], state_got.at[source], state_send.at[sp], state_recv.at[source],
                {"sp": source},
            ).wait_recv()
        state_got[sp] = state[rows_of(sp), :]
        first_row = sp * slice_rows
        g = first_row // group_rows
        row = lax.broadcasted_iota(jnp.int32, (slice_rows, LANES), 0) + (first_row - g * group_rows)
        lane = lax.broadcasted_iota(jnp.int32, (slice_rows, LANES), 1)
        spans = ends[:, 7, :]
        shift = HEAD_SIZE.bit_length() - 1
        grown = []
        for side in range(STATE_WIDE // STATE_NARROW):
            wide_head = lax.shift_right_logical(row, shift)
            narrow_head = half + side * (narrow_rows // HEAD_SIZE) + lax.shift_right_logical(
                jnp.maximum(row - wide_rows, 0), shift
            )
            head = g * GROUP_HEADS + jnp.where(row < wide_rows, wide_head, narrow_head)
            grown.append(
                jnp.exp(
                    lax.dot_general(
                        (lane == head).astype(jnp.float32), spans, (((1,), (1,)), ((), ())),
                        precision=HIGHEST, preferred_element_type=jnp.float32,
                    )
                )
            )
        carry = jnp.zeros((slice_rows, LANES), jnp.float32)
        for source in range(sp_count):
            states_out[source] = carry.astype(jnp.bfloat16)
            factor = jnp.where(lane < STATE_NARROW, grown[0][:, source : source + 1], grown[1][:, source : source + 1])
            carry = carry * factor + state_got[source].astype(jnp.float32)
        states_in[rows_of(sp), :] = states_out[sp]
        for turn in range(1, sp_count):
            back_copy(sp, flipped(sp, turn, sp_count)).start()

    def back_copy(owner, target):
        return remote(
            states_out.at[target], states_in.at[rows_of(owner)], back_send.at[target], back_recv.at[owner],
            {"sp": target},
        )

    if owners < sp_count:
        pl.when(sp < owners)(carry_all)
    else:
        carry_all()
    feed(len(queue))

    @pl.loop(ahead, groups)
    def _(g):
        inside(g)

    gate_copy.wait()

    @pl.loop(0, owners)
    def _(owner):
        @pl.when(owner != sp)
        def _():
            back_copy(owner, sp).wait_recv()

    squares_own[...] = jnp.zeros(squares_own.shape, jnp.float32)

    @pl.loop(0, groups)
    def _(g):
        cols = value_cols(g)
        by_row, by_col, _ = heads_of(g)
        growth = jnp.exp(by_col)
        base = pl.multiple_of(g * group_rows, 8)
        wide_in = states_in[pl.ds(base, wide_rows), :]
        narrow_in = states_in[pl.ds(base + wide_rows, narrow_rows), :]
        reads = [
            lax.dot_general(
                keys_at(g, STATE_WIDE, STATE_WIDE), wide_in,
                (((1,), (1,)), ((), ())), preferred_element_type=jnp.float32,
            )
        ]
        for side in range(STATE_WIDE // STATE_NARROW):
            reads.append(
                lax.dot_general(
                    keys_at(g, 2 * STATE_WIDE + STATE_NARROW, STATE_NARROW),
                    narrow_in[:, side * STATE_NARROW : (side + 1) * STATE_NARROW],
                    (((1,), (1,)), ((), ())), preferred_element_type=jnp.float32,
                )
            )
        read = jnp.concatenate(reads, axis=1)
        parts = [
            read[:, head * HEAD_SIZE : (head + 1) * HEAD_SIZE] * growth[:, head : head + 1]
            for head in range(GROUP_HEADS)
        ]
        gate = gates[:, cols].astype(jnp.float32)
        gated = (local_out[:, cols] + jnp.concatenate(parts, axis=1)) * (gate * jax.nn.sigmoid(gate))
        power = gated * gated
        folded = power[:, :LANES]
        for first in range(LANES, group_cols, LANES):
            folded = folded + power[:, first : first + LANES]
        squares_own[...] += lax.dot_general(
            jnp.ones((8, LANES), jnp.float32), folded, (((1,), (1,)), ((), ())),
            precision=HIGHEST, preferred_element_type=jnp.float32,
        )
        gained[:, cols] = (gated * mix_gain[:, cols]).astype(jnp.bfloat16)

    for step in range(1, tp_count):
        go(remote(squares_own, squares_in.at[step - 1], square_send.at[step - 1], square_recv.at[step - 1], siblings[step - 1]))
    weight_copy.wait()
    wide_step = min(256, rows)

    @pl.loop(0, features // wide_step)
    def _(index):
        block = pl.ds(pl.multiple_of(index * wide_step, LANES), wide_step)
        product = jnp.dot(gained[...], weight[:, block], preferred_element_type=jnp.float32)
        partial[block, :] = jnp.transpose(product).astype(jnp.bfloat16)

    sums = []
    for step in range(1, tp_count):
        peer = pl.ds(pl.multiple_of((tp + step) % tp_count * rows, TILE), rows)
        copy = remote(
            partial.at[peer], partial_in.at[step - 1], sum_send.at[step - 1], sum_recv.at[step - 1], siblings[step - 1]
        )
        go(copy)
        sums.append(copy)
    square = squares_own[0:1, :]
    for step in range(1, tp_count):
        remote(squares_own, squares_in.at[step - 1], square_send.at[step - 1], square_recv.at[step - 1], siblings[step - 1]).wait_recv()
        square = square + squares_in[step - 1, 0:1, :]
    inverse = lax.rsqrt(square / (inputs.shape[1] * tp_count) + NORM_FLOOR)
    own_rows = pl.ds(pl.multiple_of(tp * rows, TILE), rows)
    summed = partial[own_rows, :].astype(jnp.float32)
    for step in range(1, tp_count):
        sums[step - 1].wait_recv()
        summed = summed + partial_in[step - 1].astype(jnp.float32)
    merged[...] = (residual[...].astype(jnp.float32) + summed * inverse).astype(jnp.bfloat16)

    for turn in range(1, sp_count):
        both_block(turn).wait_recv()
    both_copy.wait()
    for copy in started:
        copy.wait_send()

    @pl.loop(0, owners)
    def _(owner):
        @pl.when(owner != sp)
        def _():
            state_copy(owner, rows_of(owner)).wait_send()

    def back_done():
        for turn in range(1, sp_count):
            back_copy(sp, flipped(sp, turn, sp_count)).wait_send()

    if owners < sp_count:
        pl.when(sp < owners)(back_done)
    else:
        back_done()


def mixed_tokens(
    values, keys, gates, time_step, decay_rate, skip, conv_values, conv_keys, mix_gain,
    weight, residual, both, span,
):
    sp_count, tp_count = lax.axis_size("sp"), lax.axis_size("tp")
    row_count, inner = values.shape
    rows = residual.shape[0]
    head_count = time_step.shape[0]
    groups = head_count // GROUP_HEADS
    features = weight.shape[1]
    half_rows = GROUP_HEADS // 2 * HEAD_SIZE
    state_rows = groups * (half_rows + half_rows * STATE_NARROW // STATE_WIDE)
    slice_rows = max(8, state_rows // sp_count)
    owners = state_rows // slice_rows
    bf, f32 = jnp.bfloat16, jnp.float32
    dma = pltpu.SemaphoreType.DMA
    near = pl.BlockSpec(memory_space=pltpu.VMEM)
    far = pl.BlockSpec(memory_space=pltpu.MemorySpace.HBM)
    tp_others, others = tp_count - 1, sp_count - 1
    return pl.pallas_call(
        functools.partial(token_mixer, sp_count, tp_count, span),
        in_specs=[near, near, far, near, near, near, near, near, near, far, near, far],
        out_specs=[near, far],
        out_shape=[
            jax.ShapeDtypeStruct((rows, row_count), bf),
            jax.ShapeDtypeStruct((sp_count,) + both.shape[1:], bf),
        ],
        scratch_shapes=[
            pltpu.VMEM((row_count, inner), bf),
            pltpu.VMEM(weight.shape, bf),
            pltpu.VMEM((TILE, inner), bf),
            pltpu.VMEM((TILE, keys.shape[1]), bf),
            pltpu.VMEM((head_count, row_count), f32),
            pltpu.VMEM((head_count, row_count), f32),
            pltpu.VMEM((row_count, inner), f32),
            pltpu.VMEM((groups, row_count, keys.shape[1] // groups), bf),
            pltpu.VMEM((row_count, inner), f32),
            pltpu.VMEM((row_count, inner), bf),
            pltpu.VMEM((sp_count * slice_rows, LANES), bf),
            pltpu.VMEM((sp_count, slice_rows, LANES), bf),
            pltpu.VMEM((sp_count, slice_rows, LANES), bf),
            pltpu.VMEM((sp_count * slice_rows, LANES), bf),
            pltpu.VMEM((8, LANES), f32),
            pltpu.VMEM((sp_count, 8, LANES), f32),
            pltpu.VMEM((8, row_count), f32),
            pltpu.VMEM((tp_others, 8, row_count), f32),
            pltpu.VMEM((features, row_count), bf),
            pltpu.VMEM((tp_others, rows, row_count), bf),
            dma((3,)),
            dma((2,)),
            dma((2,)),
            dma((others,)),
            dma((others,)),
            dma((sp_count,)),
            dma((sp_count,)),
            dma((sp_count,)),
            dma((sp_count,)),
            dma((tp_others,)),
            dma((tp_others,)),
            dma((tp_others,)),
            dma((tp_others,)),
            dma((others,)),
            dma((others,)),
        ],
        compiler_params=pltpu.CompilerParams(
            collective_id=2, has_side_effects=True, vmem_limit_bytes=VMEM_LIMIT
        ),
        cost_estimate=pl.CostEstimate(flops=10**11, bytes_accessed=10**7, transcendentals=10**6),
        name="token_mixer",
    )(
        values, keys, gates, time_step, decay_rate, skip, conv_values, conv_keys, mix_gain,
        weight, residual, both,
    )


def row_parts(rows, count):
    bounds = [rows * part // count // TILE * TILE for part in range(count)] + [rows]
    return [slice(first, last) for first, last in zip(bounds[:-1], bounds[1:])]


def channel_mixer(
    sp_count, tp_count, span,
    merged, both_rows, down_blocks, gain, taps,
    out,
    wide, both_cols, down_rows, both_pre, edges, edge_out, edge_in, tap_wide, hidden,
    partial, tp_in, total, fold_a, fold_b, fold_c,
    own_sems, spread_send, spread_recv, side_send, side_recv, edge_send, edge_recv,
    sum_send, sum_recv, fold_send, fold_recv,
):
    rows, row_count = merged.shape
    width = both_cols.shape[0]
    quarter = width // 2
    features = both_cols.shape[1]
    sp = lax.axis_index("sp")
    tp = lax.axis_index("tp")
    place = sp % span
    base = sp - place
    own_rows = pl.ds(pl.multiple_of(tp * rows, TILE), rows)
    bits = [1 << i for i in range(span.bit_length() - 1)]
    turns = sorted(range(span), key=lambda turn: (turn.bit_count(), turn))
    slot = {turn: i for i, turn in enumerate(turns)}
    orders = [bits[i:] + bits[:i] for i in range(len(bits))]
    parts = row_parts(rows, len(bits))
    after = (sp + span) % sp_count
    behind = (sp + sp_count - span) % sp_count

    def member(turn):
        return {"sp": base + flipped(place, turn, span)}

    def sibling(step):
        return {"tp": (tp + step) % tp_count}

    barrier = pltpu.get_barrier_semaphore()
    greeted = [member(bit) for bit in bits] + [sibling(step) for step in range(1, tp_count)]
    if span < sp_count:
        greeted += [{"sp": after}, {"sp": behind}]
    for peer in greeted:
        pl.semaphore_signal(barrier, inc=1, device_id=peer, device_id_type=MESH)

    own_copy = pltpu.make_async_copy(merged, wide.at[0, own_rows], own_sems)
    own_copy.start()
    own_copy.wait()
    pl.semaphore_wait(barrier, len(greeted))

    def spread(part, bit, turn):
        place_rows = pl.ds(pl.multiple_of(tp * rows + parts[part].start, TILE), parts[part].stop - parts[part].start)
        index = slot[turn ^ bit] - 1
        return pltpu.make_async_remote_copy(
            src_ref=wide.at[slot[turn], place_rows],
            dst_ref=wide.at[slot[turn ^ bit], place_rows],
            send_sem=spread_send.at[part, index],
            recv_sem=spread_recv.at[part, index],
            device_id=member(bit),
            device_id_type=MESH,
        )

    def side(turn, step):
        return pltpu.make_async_remote_copy(
            src_ref=wide.at[slot[turn], own_rows],
            dst_ref=wide.at[slot[turn], own_rows],
            send_sem=side_send.at[slot[turn], step - 1],
            recv_sem=side_recv.at[slot[turn], step - 1],
            device_id=sibling(step),
            device_id_type=MESH,
        )

    started = []

    def go(copy):
        copy.start()
        started.append(copy)

    def arrived(part, turn):
        order = orders[part]
        last = [bit for bit in order if turn & bit][-1]
        spread(part, last, turn ^ last).wait_recv()

    def onward(part, turn):
        order = orders[part]
        reach = max([-1] + [i for i, bit in enumerate(order) if turn & bit])
        for bit in order[reach + 1 :]:
            go(spread(part, bit, turn))

    for position in range(len(bits)):
        for part in range(len(bits)):
            go(spread(part, orders[part][position], 0))

    def to_sides(turn):
        for step in range(1, tp_count):
            go(side(turn, step))

    def from_sides(turn):
        for step in range(1, tp_count):
            side(turn, step).wait_recv()

    to_sides(0)

    chunk = 128
    for first in range(0, features, chunk):
        cols = slice(first, first + chunk)
        block = jnp.transpose(both_rows[cols, :].astype(jnp.float32))
        both_cols[:, cols] = (block * gain[:, cols]).astype(jnp.bfloat16)
    count, _, narrow = down_blocks.shape

    @pl.loop(0, count)
    def _(index):
        block = jnp.transpose(down_blocks[index].astype(jnp.float32))
        down_rows[pl.ds(pl.multiple_of(index * narrow, narrow), narrow), :] = block.astype(jnp.bfloat16)

    for tap in range(taps.shape[1]):
        tap_wide[tap] = jnp.broadcast_to(taps[:, tap : tap + 1], (width, LANES))

    def project(index, turn):
        columns = wide[index]
        squares = jnp.zeros((8, row_count), jnp.float32)
        for first in range(0, features, 256):
            piece = columns[first : first + 256].astype(jnp.float32)
            squares = squares + jnp.sum((piece * piece).reshape(-1, 8, row_count), axis=0)
        mean = jnp.sum(squares, axis=0, keepdims=True) / features
        scale = lax.rsqrt(mean + NORM_FLOOR)
        pre = jnp.dot(both_cols[...], columns, preferred_element_type=jnp.float32) * scale
        both_pre[index] = pre.astype(jnp.bfloat16)
        edges[1 + flipped(place, turn, span)] = pre[:, row_count - LANES :].astype(jnp.bfloat16)

    from_sides(0)
    project(0, 0)
    events = []
    for part in range(len(bits)):
        for turn in turns[1:]:
            order = orders[part]
            key = [i for i, bit in enumerate(order) if turn & bit]
            events.append((max(key), len(key), key, part, turn))
    waiting = {turn: len(bits) for turn in turns[1:]}
    pending = []
    for _, _, _, part, turn in sorted(events):
        arrived(part, turn)
        onward(part, turn)
        waiting[turn] -= 1
        if waiting[turn] == 0:
            to_sides(turn)
            pending.append(turn)
            if len(pending) > 1:
                done = pending.pop(0)
                from_sides(done)
                project(slot[done], done)
    for done in pending:
        from_sides(done)
        project(slot[done], done)

    if span < sp_count:
        last = jnp.transpose(edges[span].astype(jnp.float32))
        edge_out[...] = last[LANES - TILE :, :].astype(jnp.bfloat16)
        edge_copy = pltpu.make_async_remote_copy(
            src_ref=edge_out, dst_ref=edge_in, send_sem=edge_send, recv_sem=edge_recv,
            device_id={"sp": after}, device_id_type=MESH,
        )
        edge_copy.start()
    edges[0] = jnp.zeros(edges.shape[1:], edges.dtype)

    lane = lax.broadcasted_iota(jnp.int32, (quarter, LANES), 1)

    def taps_of(index, spot):
        for first in range(0, row_count, LANES):
            sums = []
            for kind in range(2):
                own = slice(kind * quarter, (kind + 1) * quarter)
                now = both_pre[index, own, first : first + LANES].astype(jnp.float32)
                if first:
                    past = both_pre[index, own, first - LANES : first].astype(jnp.float32)
                else:
                    past = edges[spot, own, :].astype(jnp.float32)
                tap_count = taps.shape[1]
                summed = tap_wide[tap_count - 1, own, :] * now
                for back in range(1, tap_count):
                    moved = jnp.where(lane < back, pltpu.roll(past, back, 1), pltpu.roll(now, back, 1))
                    summed = summed + tap_wide[tap_count - 1 - back, own, :] * moved
                sums.append(summed)
            value = sums[0] * jax.nn.sigmoid(sums[0]) * sums[1]
            hidden[index, :, first : first + LANES] = value.astype(jnp.bfloat16)

    for turn in turns:
        taps_of(slot[turn], flipped(place, turn, span))
    if span < sp_count:
        edge_copy.wait()
        last = jnp.transpose(edge_in[...].astype(jnp.float32))
        own_edge = jnp.where(base == 0, 0.0, last)
        edges[0, :, LANES - TILE :] = own_edge.astype(jnp.bfloat16)
        for turn in turns:
            @pl.when(flipped(place, turn, span) == 0)
            def _():
                taps_of(slot[turn], 0)

    def to_sum(turn, step):
        peer = pl.ds(pl.multiple_of((tp + step) % tp_count * rows, TILE), rows)
        return pltpu.make_async_remote_copy(
            src_ref=partial.at[slot[turn], peer],
            dst_ref=tp_in.at[slot[turn], step - 1],
            send_sem=sum_send.at[slot[turn], step - 1],
            recv_sem=sum_recv.at[slot[turn], step - 1],
            device_id=sibling(step),
            device_id_type=MESH,
        )

    folds = (fold_a, fold_b, fold_c)

    def fold(part, stage, turn):
        bit = orders[part][stage]
        here = slot[turn ^ bit]
        return pltpu.make_async_remote_copy(
            src_ref=total.at[slot[turn], parts[part]],
            dst_ref=folds[stage].at[here, parts[part]],
            send_sem=fold_send.at[part, slot[turn] - 1],
            recv_sem=fold_recv.at[part, stage, here],
            device_id=member(bit),
            device_id_type=MESH,
        )

    def stage_of(part, turn):
        return min(i for i, bit in enumerate(orders[part]) if turn & bit)

    def multiply(turn):
        step_rows = min(512, features)
        for first in range(0, features, step_rows):
            block = slice(first, first + step_rows)
            partial[slot[turn], block] = jnp.dot(
                down_rows[block, :], hidden[slot[turn]], preferred_element_type=jnp.float32
            ).astype(jnp.bfloat16)
        for step in range(1, tp_count):
            go(to_sum(turn, step))

    def add_up(turn):
        summed = partial[slot[turn], own_rows].astype(jnp.float32)
        for step in range(1, tp_count):
            to_sum(turn, step).wait_recv()
            summed = summed + tp_in[slot[turn], step - 1].astype(jnp.float32)
        total[slot[turn]] = summed.astype(jnp.bfloat16)
        if turn:
            for part in range(len(bits)):
                if stage_of(part, turn) == 0:
                    go(fold(part, 0, turn))

    line = turns[::-1]
    for position, turn in enumerate(line):
        multiply(turn)
        if position:
            add_up(line[position - 1])
    add_up(line[-1])
    for stage in range(len(bits)):
        for part in range(len(bits)):
            order = orders[part]
            left = [turn for turn in turns if not any(turn & bit for bit in order[: stage + 1])]
            for turn in sorted(left, key=lambda turn: -turn.bit_count()):
                fold(part, stage, turn ^ order[stage]).wait_recv()
                summed = total[slot[turn], parts[part]].astype(jnp.float32) + folds[stage][
                    slot[turn], parts[part]
                ].astype(jnp.float32)
                if turn:
                    total[slot[turn], parts[part]] = summed.astype(jnp.bfloat16)
                    if stage_of(part, turn) == stage + 1:
                        go(fold(part, stage + 1, turn))
                elif stage + 1 < len(bits):
                    total[0, parts[part]] = summed.astype(jnp.bfloat16)
                else:
                    out[parts[part], :] = (merged[parts[part], :].astype(jnp.float32) + summed).astype(jnp.bfloat16)
    for copy in started:
        copy.wait_send()


def mixed_channels(merged, both_rows, down_blocks, gain, taps, span):
    rows, row_count = merged.shape
    sp_count, tp_count = lax.axis_size("sp"), lax.axis_size("tp")
    features, width = both_rows.shape
    quarter = width // 2
    levels = span.bit_length() - 1
    bf = jnp.bfloat16
    dma = pltpu.SemaphoreType.DMA
    vmem = pl.BlockSpec(memory_space=pltpu.VMEM)
    return pl.pallas_call(
        functools.partial(channel_mixer, sp_count, tp_count, span),
        in_specs=[vmem] * 5,
        out_specs=vmem,
        out_shape=jax.ShapeDtypeStruct((rows, row_count), bf),
        scratch_shapes=[
            pltpu.VMEM((span, features, row_count), bf),
            pltpu.VMEM((width, features), bf),
            pltpu.VMEM((features, quarter), bf),
            pltpu.VMEM((span, width, row_count), bf),
            pltpu.VMEM((span + 1, width, LANES), bf),
            pltpu.VMEM((TILE, width), bf),
            pltpu.VMEM((TILE, width), bf),
            pltpu.VMEM((taps.shape[1], width, LANES), jnp.float32),
            pltpu.VMEM((span, quarter, row_count), bf),
            pltpu.VMEM((span, features, row_count), bf),
            pltpu.VMEM((span, tp_count - 1, rows, row_count), bf),
            pltpu.VMEM((span, rows, row_count), bf),
            pltpu.VMEM((span, rows, row_count), bf),
            pltpu.VMEM((4, rows, row_count), bf),
            pltpu.VMEM((1, rows, row_count), bf),
            dma,
            dma((levels, span - 1)),
            dma((levels, span - 1)),
            dma((span, tp_count - 1)),
            dma((span, tp_count - 1)),
            dma,
            dma,
            dma((span, tp_count - 1)),
            dma((span, tp_count - 1)),
            dma((levels, span - 1)),
            dma((levels, levels, span)),
        ],
        compiler_params=pltpu.CompilerParams(
            collective_id=1, has_side_effects=True, vmem_limit_bytes=VMEM_LIMIT
        ),
        cost_estimate=pl.CostEstimate(flops=10**11, bytes_accessed=10**7, transcendentals=10**6),
        name="channel_mixer",
    )(merged, both_rows, down_blocks, gain, taps)


def local(
    residual,
    values,
    gate_input,
    group_keys,
    time_step,
    decay_rate,
    skip_gain,
    conv_values,
    conv_keys,
    mix_gain,
    out_weight,
    norm_gain,
    hidden_gate,
    hidden_up,
    hidden_conv,
    hidden_down,
):
    sp_count = lax.axis_size("sp")
    span = min(SPAN, sp_count)
    member = lax.axis_index("sp") % span
    rows, hidden_cols = hidden_gate.shape
    quarter = hidden_cols // span
    gates = hidden_gate.reshape(rows, span, quarter)
    ups = hidden_up.reshape(rows, span, quarter)
    both = jnp.transpose(jnp.concatenate([gates, ups], axis=2), (1, 0, 2))
    merged, both_rows = mixed_tokens(
        values, group_keys, gate_input, time_step, decay_rate[:, None],
        jnp.repeat(skip_gain, HEAD_SIZE)[None, :], conv_values, conv_keys, mix_gain[None, :],
        out_weight, residual, both, span,
    )
    down = hidden_down.reshape(span, quarter, hidden_down.shape[1])
    down = jnp.concatenate([down] * (sp_count // span), axis=0)
    down, merged = lax.optimization_barrier((down, merged))
    down_blocks = lax.all_to_all(down, "sp", 0, 0, tiled=True)
    own_taps = lax.dynamic_slice_in_dim(hidden_conv, member * quarter, quarter, 2)
    own_taps = jnp.transpose(own_taps, (0, 2, 1)).reshape(2 * quarter, -1).astype(jnp.float32)
    return mixed_channels(
        merged, both_rows.reshape(sp_count * rows, 2 * quarter), down_blocks, norm_gain[None, :], own_taps, span
    )


def solution(mesh):
    in_specs = (
        P("tp", "sp"),
        P("sp", "tp"),
        P("sp", "tp"),
        P("sp", "tp"),
        P("tp", "sp"),
        P("tp"),
        P("tp"),
        P(None, "tp"),
        P(None, "tp"),
        P("tp"),
        P("tp", None),
        P(),
        P("sp", "tp"),
        P("sp", "tp"),
        P(None, None, "tp"),
        P("tp", "sp"),
    )
    out_specs = P("tp", "sp")
    return jax.shard_map(local, mesh=mesh, in_specs=in_specs, out_specs=out_specs, check_vma=False)
```

```python
import functools

import jax
import jax.numpy as jnp
from jax import lax
from jax.experimental import pallas as pl
from jax.experimental.pallas import tpu as pltpu
from jax.sharding import PartitionSpec as P

GROUP_HEADS = 8
HEAD_SIZE = 64
STATE_WIDE = 128
STATE_NARROW = 64

NORM_FLOOR = 0.1
SPAN = 8
EDGE = 8
TILE = 16
LANES = 128
FEEDS = ((1, 2), (1, 2), (1, 1), (0, 1), (0, 1), (1, 0))
EVENT_FEEDS = {position: (1, 1) for position in range(3, 21)}
VMEM_LIMIT = 63 * 2**20
MESH = pl.DeviceIdType.MESH
HIGHEST = lax.Precision.HIGHEST


def flipped(place, turn, count):
    result = 0
    bit = 1
    while bit < count:
        own = (place // bit) % 2
        result = result + bit * (own + (turn // bit) % 2 * (1 - 2 * own))
        bit *= 2
    return result


def silu_taps(before, rows, taps):
    joined = jnp.concatenate([before.astype(jnp.float32), rows.astype(jnp.float32)], axis=0)
    count = rows.shape[0]
    first = before.shape[0] - taps.shape[0] + 1
    summed = taps[0:1].astype(jnp.float32) * joined[first : first + count]
    for tap in range(1, taps.shape[0]):
        summed = summed + taps[tap : tap + 1].astype(jnp.float32) * joined[
            first + tap : first + tap + count
        ]
    return summed * jax.nn.sigmoid(summed)


def causal_rows(value, count):
    row = lax.broadcasted_iota(jnp.int32, (count, count), 0)
    col = lax.broadcasted_iota(jnp.int32, (count, count), 1)
    return jnp.where(row >= col, value, -jnp.inf)


def row_parts(rows, count):
    bounds = [rows * part // count // TILE * TILE for part in range(count)] + [rows]
    return [slice(first, last) for first, last in zip(bounds[:-1], bounds[1:])]


def layer_kernel(
    sp_count, tp_count, span,
    values, keys, gates_far, time_step, decay_rate, skip, conv_values, conv_keys, mix_gain,
    weight_far, residual, both_far, down_far, gain, taps,
    out,
    gates, slab, values_tail, keys_tail, run, delta, inputs, key_rows, local_out, gained,
    state, state_got, states_out, states_in, ends_own, ends, squares_own, squares_in,
    mixed, mixed_in, both_got, down_got,
    wide, both_cols, down_rows, both_pre, edges, edge_out, edge_in, tap_wide, hidden,
    tp_in, total, fold_a, fold_b, fold_c,
    local_sems, weight_sems, tail_send, tail_recv, ends_send, ends_recv, state_send, state_recv,
    back_send, back_recv, square_send, square_recv, mix_send, mix_recv, both_send, both_recv,
    down_send, down_recv, spread_send, spread_recv, side_send, side_recv, edge_send, edge_recv,
    sum_send, sum_recv, fold_send, fold_recv,
):
    sp = lax.axis_index("sp")
    tp = lax.axis_index("tp")
    row_count = values.shape[0]
    head_count = time_step.shape[0]
    groups = head_count // GROUP_HEADS
    half = GROUP_HEADS // 2
    key_cols = 2 * STATE_WIDE + 2 * STATE_NARROW
    group_cols = GROUP_HEADS * HEAD_SIZE
    wide_rows = half * HEAD_SIZE
    narrow_rows = wide_rows * STATE_NARROW // STATE_WIDE
    group_rows = wide_rows + narrow_rows
    slice_rows = states_out.shape[1]
    owners = groups * group_rows // slice_rows
    rows = residual.shape[0]
    features = wide.shape[1]
    place = sp % span
    base_place = sp - place

    gate_copy = pltpu.make_async_copy(gates_far, gates, local_sems.at[0])
    gate_copy.start()
    weight_rows = weight_far.shape[0]
    weight_copies = []
    for index in range(features // row_count):
        copy = pltpu.make_async_copy(
            weight_far.at[:, index * row_count : (index + 1) * row_count],
            slab.at[index, 0:weight_rows],
            weight_sems.at[index],
        )
        copy.start()
        weight_copies.append(copy)
    both_copy = pltpu.make_async_copy(both_far.at[place], both_got.at[sp], local_sems.at[1])
    both_copy.start()
    down_copy = pltpu.make_async_copy(down_far.at[place], down_got.at[sp], local_sems.at[2])
    down_copy.start()

    others = [{"sp": flipped(sp, turn, sp_count)} for turn in range(1, sp_count)]
    siblings = [{"tp": (tp + step) % tp_count} for step in range(1, tp_count)]
    barrier = pltpu.get_barrier_semaphore()
    for peer in others + siblings:
        pl.semaphore_signal(barrier, inc=1, device_id=peer, device_id_type=MESH)

    deltas = jnp.maximum(time_step[...], 0.0) + jnp.log1p(jnp.exp(-jnp.abs(time_step[...])))
    delta[...] = deltas
    upto = lax.broadcasted_iota(jnp.int32, (row_count, row_count), 0) <= lax.broadcasted_iota(
        jnp.int32, (row_count, row_count), 1
    )
    running = jnp.dot(
        -decay_rate[...] * deltas, upto.astype(jnp.float32),
        precision=HIGHEST, preferred_element_type=jnp.float32,
    )
    run[...] = running
    tail_heads = jnp.concatenate(
        [running[:, row_count - LANES :], jnp.zeros((LANES - head_count, LANES), jnp.float32)], axis=0
    )
    last_rows = jnp.transpose(tail_heads)[LANES - 8 :, :]
    ends_own[...] = last_rows
    ends[sp] = last_rows

    pl.semaphore_wait(barrier, len(others) + len(siblings))

    started = []

    def go(copy):
        copy.start()
        started.append(copy)

    def remote(source, target, send, recv, peer):
        return pltpu.make_async_remote_copy(
            src_ref=source, dst_ref=target, send_sem=send, recv_sem=recv,
            device_id=peer, device_id_type=MESH,
        )

    after = {"sp": (sp + 1) % sp_count}
    last = slice(row_count - TILE, row_count)
    tails = [
        remote(values.at[last], values_tail, tail_send.at[0], tail_recv.at[0], after),
        remote(keys.at[last], keys_tail, tail_send.at[1], tail_recv.at[1], after),
    ]
    for copy in tails:
        go(copy)

    def both_block(turn):
        peer = flipped(sp, turn, sp_count)
        return remote(
            both_far.at[peer % span], both_got.at[sp], both_send.at[turn - 1], both_recv.at[turn - 1],
            {"sp": peer},
        )

    def down_block(turn):
        peer = flipped(sp, turn, sp_count)
        return remote(
            down_far.at[peer % span], down_got.at[sp], down_send.at[turn - 1], down_recv.at[turn - 1],
            {"sp": peer},
        )

    far_turns = list(range(span, sp_count))
    near_turns = list(range(1, span))
    queue = [(both_block, far_turns), (both_block, near_turns), (down_block, far_turns), (down_block, near_turns)]
    queue = [(kind, list(line)) for kind, line in queue]

    def feed(far_count, near_count):
        for first, count in ((0, far_count), (1, near_count)):
            for _ in range(count):
                kind, line = queue[first] if queue[first][1] else queue[first + 2]
                if line:
                    go(kind(line.pop(0)))

    for turn in range(1, sp_count):
        peer = {"sp": flipped(sp, turn, sp_count)}
        go(remote(ends_own, ends.at[sp], ends_send.at[turn - 1], ends_recv.at[turn - 1], peer))
    feed(*FEEDS[0])
    for copy in tails:
        copy.wait_recv()

    def heads_of(g):
        spot = pl.ds(pl.multiple_of(g * GROUP_HEADS, GROUP_HEADS), GROUP_HEADS)
        by_row = run[spot, :]
        return by_row, jnp.transpose(by_row), jnp.transpose(delta[spot, :])

    def value_cols(g):
        return pl.ds(pl.multiple_of(g * group_cols, LANES), group_cols)

    def keys_at(g, first, width):
        return key_rows[g, :, first : first + width]

    kinds = ((0, STATE_WIDE), (2 * STATE_WIDE, STATE_NARROW))

    def state_copy(owner, own_slice):
        return remote(
            state.at[own_slice], state_got.at[sp], state_send.at[owner], state_recv.at[sp], {"sp": owner}
        )

    def rows_of(owner):
        return pl.ds(pl.multiple_of(owner * slice_rows, 8), slice_rows)

    @pl.loop(0, groups)
    def _(g):
        cols = value_cols(g)
        key_span = pl.ds(pl.multiple_of(g * key_cols, LANES), key_cols)
        first = sp == 0
        before = jnp.where(first, 0.0, values_tail[TILE - 8 :, cols].astype(jnp.float32))
        inner = silu_taps(before, values[:, cols], conv_values[:, cols])
        inputs[:, cols] = inner
        before = jnp.where(first, 0.0, keys_tail[TILE - 8 :, key_span].astype(jnp.float32))
        made = silu_taps(before, keys[:, key_span], conv_keys[:, key_span]).astype(jnp.bfloat16)
        key_rows[g] = made
        by_row, by_col, deltas = heads_of(g)
        states = []
        for kind, (first_col, width) in enumerate(kinds):
            scaled = []
            for head in range(kind * half, (kind + 1) * half):
                own = slice(head * HEAD_SIZE, (head + 1) * HEAD_SIZE)
                to_end = jnp.exp(by_row[head : head + 1, row_count - 1 :] - by_col[:, head : head + 1])
                scaled.append((inner[:, own] * (deltas[:, head : head + 1] * to_end)).astype(jnp.bfloat16))
            states.append(
                lax.dot_general(
                    jnp.concatenate(scaled, axis=1),
                    made[:, first_col : first_col + width],
                    (((0,), (0,)), ((), ())),
                    preferred_element_type=jnp.float32,
                ).astype(jnp.bfloat16)
            )
        base = pl.multiple_of(g * group_rows, 8)
        state[pl.ds(base, wide_rows), :] = states[0]
        fold = STATE_WIDE // STATE_NARROW
        state[pl.ds(base + wide_rows, narrow_rows), :] = jnp.concatenate(
            [states[1][i * narrow_rows : (i + 1) * narrow_rows] for i in range(fold)], axis=1
        )
        per_group = group_rows // slice_rows

        @pl.loop(0, per_group)
        def _(index):
            owner = g * per_group + index

            @pl.when(owner != sp)
            def _():
                state_copy(owner, rows_of(owner)).start()

    feed(*FEEDS[1])

    def inside(g):
        cols = value_cols(g)
        by_row, by_col, deltas = heads_of(g)
        inner = inputs[:, cols]
        outs = []
        for kind, (first_col, width) in enumerate(kinds):
            scores = lax.dot_general(
                keys_at(g, first_col + width, width), keys_at(g, first_col, width),
                (((1,), (1,)), ((), ())), preferred_element_type=jnp.float32,
            )
            for head in range(kind * half, (kind + 1) * half):
                own = slice(head * HEAD_SIZE, (head + 1) * HEAD_SIZE)
                gap = causal_rows(by_col[:, head : head + 1] - by_row[head : head + 1, :], row_count)
                mixing = (scores * jnp.exp(gap)).astype(jnp.bfloat16)
                weighted = (inner[:, own] * deltas[:, head : head + 1]).astype(jnp.bfloat16)
                outs.append(jnp.dot(mixing, weighted, preferred_element_type=jnp.float32))
        local_out[:, cols] = jnp.concatenate(outs, axis=1) + inner * skip[:, cols]

    ahead = (groups + 1) // 2
    @pl.loop(0, ahead)
    def _(g):
        inside(g)

    for turn in range(1, sp_count):
        peer = {"sp": flipped(sp, turn, sp_count)}
        remote(ends_own, ends.at[sp], ends_send.at[turn - 1], ends_recv.at[turn - 1], peer).wait_recv()

    def carry_all():
        for turn in range(1, sp_count):
            source = flipped(sp, turn, sp_count)
            remote(
                state.at[rows_of(sp)], state_got.at[source], state_send.at[sp], state_recv.at[source],
                {"sp": source},
            ).wait_recv()
        state_got[sp] = state[rows_of(sp), :]
        first_row = sp * slice_rows
        g = first_row // group_rows
        row = lax.broadcasted_iota(jnp.int32, (slice_rows, LANES), 0) + (first_row - g * group_rows)
        lane = lax.broadcasted_iota(jnp.int32, (slice_rows, LANES), 1)
        spans = ends[:, 7, :]
        shift = HEAD_SIZE.bit_length() - 1
        grown = []
        for side in range(STATE_WIDE // STATE_NARROW):
            wide_head = lax.shift_right_logical(row, shift)
            narrow_head = half + side * (narrow_rows // HEAD_SIZE) + lax.shift_right_logical(
                jnp.maximum(row - wide_rows, 0), shift
            )
            head = g * GROUP_HEADS + jnp.where(row < wide_rows, wide_head, narrow_head)
            grown.append(
                jnp.exp(
                    lax.dot_general(
                        (lane == head).astype(jnp.float32), spans, (((1,), (1,)), ((), ())),
                        precision=HIGHEST, preferred_element_type=jnp.float32,
                    )
                )
            )
        carry = jnp.zeros((slice_rows, LANES), jnp.float32)
        for source in range(sp_count):
            states_out[source] = carry.astype(jnp.bfloat16)
            factor = jnp.where(lane < STATE_NARROW, grown[0][:, source : source + 1], grown[1][:, source : source + 1])
            carry = carry * factor + state_got[source].astype(jnp.float32)
        states_in[rows_of(sp), :] = states_out[sp]
        for turn in range(1, sp_count):
            back_copy(sp, flipped(sp, turn, sp_count)).start()

    def back_copy(owner, target):
        return remote(
            states_out.at[target], states_in.at[rows_of(owner)], back_send.at[target], back_recv.at[owner],
            {"sp": target},
        )

    if owners < sp_count:
        pl.when(sp < owners)(carry_all)
    else:
        carry_all()
    feed(*FEEDS[2])

    @pl.loop(ahead, groups)
    def _(g):
        inside(g)

    gate_copy.wait()
    feed(*FEEDS[3])

    @pl.loop(0, owners)
    def _(owner):
        @pl.when(owner != sp)
        def _():
            back_copy(owner, sp).wait_recv()

    squares_own[...] = jnp.zeros(squares_own.shape, jnp.float32)

    @pl.loop(0, groups)
    def _(g):
        cols = value_cols(g)
        by_row, by_col, _ = heads_of(g)
        growth = jnp.exp(by_col)
        base = pl.multiple_of(g * group_rows, 8)
        wide_in = states_in[pl.ds(base, wide_rows), :]
        narrow_in = states_in[pl.ds(base + wide_rows, narrow_rows), :]
        reads = [
            lax.dot_general(
                keys_at(g, STATE_WIDE, STATE_WIDE), wide_in,
                (((1,), (1,)), ((), ())), preferred_element_type=jnp.float32,
            )
        ]
        for side in range(STATE_WIDE // STATE_NARROW):
            reads.append(
                lax.dot_general(
                    keys_at(g, 2 * STATE_WIDE + STATE_NARROW, STATE_NARROW),
                    narrow_in[:, side * STATE_NARROW : (side + 1) * STATE_NARROW],
                    (((1,), (1,)), ((), ())), preferred_element_type=jnp.float32,
                )
            )
        read = jnp.concatenate(reads, axis=1)
        parts = [
            read[:, head * HEAD_SIZE : (head + 1) * HEAD_SIZE] * growth[:, head : head + 1]
            for head in range(GROUP_HEADS)
        ]
        gate = gates[:, cols].astype(jnp.float32)
        gated = (local_out[:, cols] + jnp.concatenate(parts, axis=1)) * (gate * jax.nn.sigmoid(gate))
        power = gated * gated
        folded = power[:, :LANES]
        for first in range(LANES, group_cols, LANES):
            folded = folded + power[:, first : first + LANES]
        squares_own[...] += lax.dot_general(
            jnp.ones((8, LANES), jnp.float32), folded, (((1,), (1,)), ((), ())),
            precision=HIGHEST, preferred_element_type=jnp.float32,
        )
        gained[:, cols] = (gated * mix_gain[:, cols]).astype(jnp.bfloat16)

    for step in range(1, tp_count):
        go(remote(squares_own, squares_in.at[step - 1], square_send.at[step - 1], square_recv.at[step - 1], siblings[step - 1]))
    for index, copy in enumerate(weight_copies):
        copy.wait()
        product = jnp.dot(gained[...], slab[index, 0:weight_rows], preferred_element_type=jnp.float32)
        mixed[index * row_count : (index + 1) * row_count, :] = jnp.transpose(product).astype(jnp.bfloat16)
    feed(*FEEDS[4])

    sums = []
    for step in range(1, tp_count):
        peer = pl.ds(pl.multiple_of((tp + step) % tp_count * rows, TILE), rows)
        copy = remote(
            mixed.at[peer], mixed_in.at[step - 1], mix_send.at[step - 1], mix_recv.at[step - 1], siblings[step - 1]
        )
        go(copy)
        sums.append(copy)
    square = squares_own[0:1, :]
    for step in range(1, tp_count):
        remote(squares_own, squares_in.at[step - 1], square_send.at[step - 1], square_recv.at[step - 1], siblings[step - 1]).wait_recv()
        square = square + squares_in[step - 1, 0:1, :]
    inverse = lax.rsqrt(square / (inputs.shape[1] * tp_count) + NORM_FLOOR)
    own_rows = pl.ds(pl.multiple_of(tp * rows, TILE), rows)
    summed = mixed[own_rows, :].astype(jnp.float32)
    for step in range(1, tp_count):
        sums[step - 1].wait_recv()
        summed = summed + mixed_in[step - 1].astype(jnp.float32)
    wide[0, own_rows] = (residual[...].astype(jnp.float32) + summed * inverse).astype(jnp.bfloat16)

    width = both_cols.shape[0]
    quarter = width // 2
    bits = [1 << i for i in range(span.bit_length() - 1)]
    turns = sorted(range(span), key=lambda turn: (turn.bit_count(), turn))
    slot = {turn: i for i, turn in enumerate(turns)}
    orders = [bits[i:] + bits[:i] for i in range(len(bits))]
    parts = row_parts(rows, len(bits))
    next_span = (sp + span) % sp_count

    def member(turn):
        return {"sp": base_place + flipped(place, turn, span)}

    def sibling(step):
        return siblings[step - 1]

    def part_rows(part):
        size = parts[part].stop - parts[part].start
        return pl.ds(pl.multiple_of(tp * rows + parts[part].start, TILE), size)

    def spread(part, bit, turn):
        place_rows = part_rows(part)
        index = slot[turn ^ bit] - 1
        return pltpu.make_async_remote_copy(
            src_ref=wide.at[slot[turn], place_rows],
            dst_ref=wide.at[slot[turn ^ bit], place_rows],
            send_sem=spread_send.at[part, index],
            recv_sem=spread_recv.at[part, index],
            device_id=member(bit),
            device_id_type=MESH,
        )

    def side(turn, step):
        return pltpu.make_async_remote_copy(
            src_ref=wide.at[slot[turn], own_rows],
            dst_ref=wide.at[slot[turn], own_rows],
            send_sem=side_send.at[slot[turn], step - 1],
            recv_sem=side_recv.at[slot[turn], step - 1],
            device_id=sibling(step),
            device_id_type=MESH,
        )

    def arrived(part, turn):
        order = orders[part]
        last = [bit for bit in order if turn & bit][-1]
        spread(part, last, turn ^ last).wait_recv()

    def onward(part, turn):
        order = orders[part]
        reach = max([-1] + [i for i, bit in enumerate(order) if turn & bit])
        for bit in order[reach + 1 :]:
            go(spread(part, bit, turn))

    for position in range(len(bits)):
        for part in range(len(bits)):
            go(spread(part, orders[part][position], 0))

    def to_sides(turn):
        for step in range(1, tp_count):
            go(side(turn, step))

    def from_sides(turn):
        for step in range(1, tp_count):
            side(turn, step).wait_recv()

    to_sides(0)
    feed(*FEEDS[5])

    def turn_both():
        both_copy.wait()
        for turn in range(1, sp_count):
            both_block(turn).wait_recv()
        chunk = 128
        for first in range(0, features, chunk):
            cols = slice(first, first + chunk)
            each = both_got.shape[1]
            block = both_got[first // each : (first + chunk) // each].reshape(chunk, width)
            block = jnp.transpose(block.astype(jnp.float32))
            both_cols[:, cols] = (block * gain[:, cols]).astype(jnp.bfloat16)

    def turn_down():
        down_copy.wait()
        for turn in range(1, sp_count):
            down_block(turn).wait_recv()
        narrow = down_got.shape[2]
        for index in range(sp_count):
            block = jnp.transpose(down_got[index].astype(jnp.float32))
            down_rows[index * narrow : (index + 1) * narrow, :] = block.astype(jnp.bfloat16)

    for tap in range(taps.shape[1]):
        tap_wide[tap] = jnp.broadcast_to(taps[:, tap : tap + 1], (width, LANES))

    def project(index, turn):
        columns = wide[index]
        squares = jnp.zeros((8, row_count), jnp.float32)
        for first in range(0, features, 256):
            piece = columns[first : first + 256].astype(jnp.float32)
            squares = squares + jnp.sum((piece * piece).reshape(-1, 8, row_count), axis=0)
        mean = jnp.sum(squares, axis=0, keepdims=True) / features
        scale = lax.rsqrt(mean + NORM_FLOOR)
        pre = jnp.dot(both_cols[...], columns, preferred_element_type=jnp.float32) * scale
        both_pre[index] = pre.astype(jnp.bfloat16)
        edges[1 + flipped(place, turn, span)] = pre[:, row_count - LANES :].astype(jnp.bfloat16)

    events = []
    for part in range(len(bits)):
        for turn in turns[1:]:
            order = orders[part]
            key = [i for i, bit in enumerate(order) if turn & bit]
            events.append((max(key), len(key), key, part, turn))
    waiting = {turn: len(bits) for turn in turns[1:]}
    for position, (_, _, _, part, turn) in enumerate(sorted(events)):
        arrived(part, turn)
        onward(part, turn)
        feed(*EVENT_FEEDS.get(position, (0, 0)))
        waiting[turn] -= 1
        if waiting[turn] == 0:
            to_sides(turn)
    feed(2 * sp_count, 2 * sp_count)
    turn_both()
    for turn in turns:
        from_sides(turn)
        project(slot[turn], turn)

    if span < sp_count:
        last = jnp.transpose(edges[span].astype(jnp.float32))
        edge_out[...] = last[LANES - TILE :, :].astype(jnp.bfloat16)
        edge_copy = pltpu.make_async_remote_copy(
            src_ref=edge_out, dst_ref=edge_in, send_sem=edge_send, recv_sem=edge_recv,
            device_id={"sp": next_span}, device_id_type=MESH,
        )
        edge_copy.start()
    edges[0] = jnp.zeros(edges.shape[1:], edges.dtype)

    lane = lax.broadcasted_iota(jnp.int32, (quarter, LANES), 1)

    def taps_of(index, spot):
        for first in range(0, row_count, LANES):
            sums = []
            for kind in range(2):
                own = slice(kind * quarter, (kind + 1) * quarter)
                now = both_pre[index, own, first : first + LANES].astype(jnp.float32)
                if first:
                    past = both_pre[index, own, first - LANES : first].astype(jnp.float32)
                else:
                    past = edges[spot, own, :].astype(jnp.float32)
                tap_count = taps.shape[1]
                summed = tap_wide[tap_count - 1, own, :] * now
                for back in range(1, tap_count):
                    moved = jnp.where(lane < back, pltpu.roll(past, back, 1), pltpu.roll(now, back, 1))
                    summed = summed + tap_wide[tap_count - 1 - back, own, :] * moved
                sums.append(summed)
            value = sums[0] * jax.nn.sigmoid(sums[0]) * sums[1]
            hidden[index, :, first : first + LANES] = value.astype(jnp.bfloat16)

    for turn in turns:
        taps_of(slot[turn], flipped(place, turn, span))
    if span < sp_count:
        edge_copy.wait()
        last = jnp.transpose(edge_in[...].astype(jnp.float32))
        own_edge = jnp.where(base_place == 0, 0.0, last)
        edges[0, :, LANES - TILE :] = own_edge.astype(jnp.bfloat16)
        for turn in turns:
            @pl.when(flipped(place, turn, span) == 0)
            def _():
                taps_of(slot[turn], 0)

    def to_sum(turn, step):
        peer = pl.ds(pl.multiple_of((tp + step) % tp_count * rows, TILE), rows)
        return pltpu.make_async_remote_copy(
            src_ref=slab.at[slot[turn], peer],
            dst_ref=tp_in.at[slot[turn], step - 1],
            send_sem=sum_send.at[slot[turn], step - 1],
            recv_sem=sum_recv.at[slot[turn], step - 1],
            device_id=sibling(step),
            device_id_type=MESH,
        )

    folds = (fold_a, fold_b, fold_c)

    def fold(part, stage, turn):
        bit = orders[part][stage]
        here = slot[turn ^ bit]
        return pltpu.make_async_remote_copy(
            src_ref=total.at[slot[turn], parts[part]],
            dst_ref=folds[stage].at[here, parts[part]],
            send_sem=fold_send.at[part, slot[turn] - 1],
            recv_sem=fold_recv.at[part, stage, here],
            device_id=member(bit),
            device_id_type=MESH,
        )

    def stage_of(part, turn):
        return min(i for i, bit in enumerate(orders[part]) if turn & bit)

    def multiply(turn):
        step_rows = min(512, features)
        for first in range(0, features, step_rows):
            block = slice(first, first + step_rows)
            slab[slot[turn], block] = jnp.dot(
                down_rows[block, :], hidden[slot[turn]], preferred_element_type=jnp.float32
            ).astype(jnp.bfloat16)
        for step in range(1, tp_count):
            go(to_sum(turn, step))

    def add_up(turn):
        summed = slab[slot[turn], own_rows].astype(jnp.float32)
        for step in range(1, tp_count):
            to_sum(turn, step).wait_recv()
            summed = summed + tp_in[slot[turn], step - 1].astype(jnp.float32)
        total[slot[turn]] = summed.astype(jnp.bfloat16)
        if turn:
            for part in range(len(bits)):
                if stage_of(part, turn) == 0:
                    go(fold(part, 0, turn))

    turn_down()
    line = turns[::-1]
    for position, turn in enumerate(line):
        multiply(turn)
        if position:
            add_up(line[position - 1])
    add_up(line[-1])
    for stage in range(len(bits)):
        for part in range(len(bits)):
            order = orders[part]
            left = [turn for turn in turns if not any(turn & bit for bit in order[: stage + 1])]
            for turn in sorted(left, key=lambda turn: -turn.bit_count()):
                fold(part, stage, turn ^ order[stage]).wait_recv()
                summed = total[slot[turn], parts[part]].astype(jnp.float32) + folds[stage][
                    slot[turn], parts[part]
                ].astype(jnp.float32)
                if turn:
                    total[slot[turn], parts[part]] = summed.astype(jnp.bfloat16)
                    if stage_of(part, turn) == stage + 1:
                        go(fold(part, stage + 1, turn))
                elif stage + 1 < len(bits):
                    total[0, parts[part]] = summed.astype(jnp.bfloat16)
                else:
                    out[parts[part], :] = (wide[0, part_rows(part)].astype(jnp.float32) + summed).astype(jnp.bfloat16)
    for copy in started:
        copy.wait_send()


    @pl.loop(0, owners)
    def _(owner):
        @pl.when(owner != sp)
        def _():
            state_copy(owner, rows_of(owner)).wait_send()

    def back_done():
        for turn in range(1, sp_count):
            back_copy(sp, flipped(sp, turn, sp_count)).wait_send()

    if owners < sp_count:
        pl.when(sp < owners)(back_done)
    else:
        back_done()


def whole_layer(
    values, keys, gates, time_step, decay_rate, skip, conv_values, conv_keys, mix_gain,
    weight, residual, both, down, gain, taps, span,
):
    sp_count, tp_count = lax.axis_size("sp"), lax.axis_size("tp")
    row_count, inner = values.shape
    rows = residual.shape[0]
    head_count = time_step.shape[0]
    groups = head_count // GROUP_HEADS
    features = weight.shape[1]
    half_rows = GROUP_HEADS // 2 * HEAD_SIZE
    state_rows = groups * (half_rows + half_rows * STATE_NARROW // STATE_WIDE)
    slice_rows = max(8, state_rows // sp_count)
    width = both.shape[2]
    quarter = width // 2
    levels = span.bit_length() - 1
    bf, f32 = jnp.bfloat16, jnp.float32
    near = pl.BlockSpec(memory_space=pltpu.VMEM)
    far = pl.BlockSpec(memory_space=pltpu.MemorySpace.HBM)
    tp_others, others = tp_count - 1, sp_count - 1
    buffers = [
        ((row_count, inner), bf),
        ((max(span, features // row_count), features, row_count), bf),
        ((TILE, inner), bf),
        ((TILE, keys.shape[1]), bf),
        ((head_count, row_count), f32),
        ((head_count, row_count), f32),
        ((row_count, inner), f32),
        ((groups, row_count, keys.shape[1] // groups), bf),
        ((row_count, inner), f32),
        ((row_count, inner), bf),
        ((sp_count * slice_rows, LANES), bf),
        ((sp_count, slice_rows, LANES), bf),
        ((sp_count, slice_rows, LANES), bf),
        ((sp_count * slice_rows, LANES), bf),
        ((8, LANES), f32),
        ((sp_count, 8, LANES), f32),
        ((8, row_count), f32),
        ((tp_others, 8, row_count), f32),
        ((features, row_count), bf),
        ((tp_others, rows, row_count), bf),
        ((sp_count,) + both.shape[1:], bf),
        ((sp_count,) + down.shape[1:], bf),
        ((span, features, row_count), bf),
        ((width, features), bf),
        ((features, quarter), bf),
        ((span, width, row_count), bf),
        ((span + 1, width, LANES), bf),
        ((TILE, width), bf),
        ((TILE, width), bf),
        ((taps.shape[1], width, LANES), f32),
        ((span, quarter, row_count), bf),
        ((span, tp_others, rows, row_count), bf),
        ((span, rows, row_count), bf),
        ((span, rows, row_count), bf),
        ((4, rows, row_count), bf),
        ((1, rows, row_count), bf),
    ]
    counts = [
        (3,), (features // row_count,), (2,), (2,), (others,), (others,), (sp_count,), (sp_count,),
        (sp_count,), (sp_count,), (tp_others,), (tp_others,), (tp_others,), (tp_others,), (others,), (others,),
        (others,), (others,), (levels, span - 1), (levels, span - 1), (span, tp_others), (span, tp_others), None, None,
        (span, tp_others), (span, tp_others), (levels, span - 1), (levels, levels, span),
    ]
    return pl.pallas_call(
        functools.partial(layer_kernel, sp_count, tp_count, span),
        in_specs=[near, near, far, near, near, near, near, near, near, far, near, far, far, near, near],
        out_specs=near,
        out_shape=jax.ShapeDtypeStruct((rows, row_count), bf),
        scratch_shapes=[pltpu.VMEM(shape, dtype) for shape, dtype in buffers]
        + [pltpu.SemaphoreType.DMA(shape) if shape else pltpu.SemaphoreType.DMA for shape in counts],
        compiler_params=pltpu.CompilerParams(
            collective_id=1, has_side_effects=True, vmem_limit_bytes=VMEM_LIMIT
        ),
        cost_estimate=pl.CostEstimate(flops=10**11, bytes_accessed=10**7, transcendentals=10**6),
        name="layer_kernel",
    )(
        values, keys, gates, time_step, decay_rate, skip, conv_values, conv_keys, mix_gain,
        weight, residual, both, down, gain, taps,
    )


def local(
    residual,
    values,
    gate_input,
    group_keys,
    time_step,
    decay_rate,
    skip_gain,
    conv_values,
    conv_keys,
    mix_gain,
    out_weight,
    norm_gain,
    hidden_gate,
    hidden_up,
    hidden_conv,
    hidden_down,
):
    sp_count = lax.axis_size("sp")
    span = min(SPAN, sp_count)
    member = lax.axis_index("sp") % span
    rows, hidden_cols = hidden_gate.shape
    quarter = hidden_cols // span
    gates = hidden_gate.reshape(rows, span, quarter)
    ups = hidden_up.reshape(rows, span, quarter)
    both = jnp.transpose(jnp.concatenate([gates, ups], axis=2), (1, 0, 2))
    down = hidden_down.reshape(span, quarter, hidden_down.shape[1])
    own_taps = lax.dynamic_slice_in_dim(hidden_conv, member * quarter, quarter, 2)
    own_taps = jnp.transpose(own_taps, (0, 2, 1)).reshape(2 * quarter, -1).astype(jnp.float32)
    return whole_layer(
        values, group_keys, gate_input, time_step, decay_rate[:, None],
        jnp.repeat(skip_gain, HEAD_SIZE)[None, :], conv_values, conv_keys, mix_gain[None, :],
        out_weight, residual, both, down, norm_gain[None, :], own_taps, span,
    )


def solution(mesh):
    in_specs = (
        P("tp", "sp"),
        P("sp", "tp"),
        P("sp", "tp"),
        P("sp", "tp"),
        P("tp", "sp"),
        P("tp"),
        P("tp"),
        P(None, "tp"),
        P(None, "tp"),
        P("tp"),
        P("tp", None),
        P(),
        P("sp", "tp"),
        P("sp", "tp"),
        P(None, None, "tp"),
        P("tp", "sp"),
    )
    out_specs = P("tp", "sp")
    return jax.shard_map(local, mesh=mesh, in_specs=in_specs, out_specs=out_specs, check_vma=False)
```

```python
import functools

import jax
import jax.numpy as jnp
from jax import lax
from jax.experimental import pallas as pl
from jax.experimental.pallas import tpu as pltpu
from jax.sharding import PartitionSpec as P

GROUP_HEADS = 8
HEAD_SIZE = 64
STATE_WIDE = 128
STATE_NARROW = 64

NORM_FLOOR = 0.1
SPAN = 8
EDGE = 8
TILE = 16
FAR_ORDER = (0, 2, 1, 2)
SHARES = (5, 5, 5)
LANES = 128
FEEDS = ((0, 3), (1, 2), (1, 2), (1, 0), (1, 0), (1, 0))
EVENT_FEEDS = {position: (1, 1) for position in range(3, 21)}
VMEM_LIMIT = 63 * 2**20
MESH = pl.DeviceIdType.MESH
HIGHEST = lax.Precision.HIGHEST


def flipped(place, turn, count):
    result = 0
    bit = 1
    while bit < count:
        own = (place // bit) % 2
        result = result + bit * (own + (turn // bit) % 2 * (1 - 2 * own))
        bit *= 2
    return result


def silu_taps(before, rows, taps):
    joined = jnp.concatenate([before.astype(jnp.float32), rows.astype(jnp.float32)], axis=0)
    count = rows.shape[0]
    first = before.shape[0] - taps.shape[0] + 1
    summed = taps[0:1].astype(jnp.float32) * joined[first : first + count]
    for tap in range(1, taps.shape[0]):
        summed = summed + taps[tap : tap + 1].astype(jnp.float32) * joined[
            first + tap : first + tap + count
        ]
    return summed * jax.nn.sigmoid(summed)


def causal_rows(value, count):
    row = lax.broadcasted_iota(jnp.int32, (count, count), 0)
    col = lax.broadcasted_iota(jnp.int32, (count, count), 1)
    return jnp.where(row >= col, value, -jnp.inf)


def row_parts(rows, shares):
    whole = sum(shares)
    bounds = [rows * sum(shares[:part]) // whole // TILE * TILE for part in range(len(shares))] + [rows]
    return [slice(first, last) for first, last in zip(bounds[:-1], bounds[1:])]


def layer_kernel(
    sp_count, tp_count, span,
    values, keys, gates_far, time_step, decay_rate, skip_gain, conv_values, conv_keys, mix_gain,
    weight_far, residual, gate_rows, up_rows, down_far, gain, taps,
    out,
    both_far,
    gates, slab, values_tail, keys_tail, run, delta, inputs, key_rows, gained,
    state, state_got, states_out, states_in, state_sum, sums_got, ends_own, ends, squares_own, squares_in,
    mixed, mixed_in, both_got, down_got,
    wide, both_cols, down_rows, both_pre, edges, edge_out, edge_in, tap_wide, hidden,
    tp_in, total, fold_a, fold_b, fold_c,
    local_sems, weight_sems, tail_send, tail_recv, ends_send, ends_recv, state_send, state_recv,
    back_send, back_recv, total_send, total_recv, square_send, square_recv, mix_send, mix_recv, both_send, both_recv,
    down_send, down_recv, spread_send, spread_recv, side_send, side_recv, edge_send, edge_recv,
    sum_send, sum_recv, fold_send, fold_recv,
):
    sp = lax.axis_index("sp")
    tp = lax.axis_index("tp")
    row_count = values.shape[0]
    head_count = time_step.shape[0]
    groups = head_count // GROUP_HEADS
    half = GROUP_HEADS // 2
    key_cols = 2 * STATE_WIDE + 2 * STATE_NARROW
    group_cols = GROUP_HEADS * HEAD_SIZE
    wide_rows = half * HEAD_SIZE
    narrow_rows = wide_rows * STATE_NARROW // STATE_WIDE
    group_rows = wide_rows + narrow_rows
    slice_rows = states_out.shape[1]
    owners = span
    span_count = sp_count // span
    group_of_spans = sp // span
    rows = residual.shape[0]
    features = wide.shape[1]
    place = sp % span
    base_place = sp - place

    gate_copy = pltpu.make_async_copy(gates_far, gates, local_sems.at[0])
    gate_copy.start()
    weight_rows = weight_far.shape[0]
    weight_copies = []
    for index in range(features // row_count):
        copy = pltpu.make_async_copy(
            weight_far.at[:, index * row_count : (index + 1) * row_count],
            slab.at[index, 0:weight_rows],
            weight_sems.at[index],
        )
        copy.start()
        weight_copies.append(copy)
    down_copy = pltpu.make_async_copy(down_far.at[place], down_got.at[sp], local_sems.at[2])
    down_copy.start()

    quarter = gate_rows.shape[1] // span
    for index in range(span):
        cols = slice(index * quarter, (index + 1) * quarter)
        both_far[index] = jnp.concatenate(
            [gate_rows[:, cols].astype(jnp.float32), up_rows[:, cols].astype(jnp.float32)], axis=1
        ).astype(jnp.bfloat16)

    others = [{"sp": flipped(sp, turn, sp_count)} for turn in range(1, sp_count)]
    siblings = [{"tp": (tp + step) % tp_count} for step in range(1, tp_count)]
    barrier = pltpu.get_barrier_semaphore()
    for peer in others + siblings:
        pl.semaphore_signal(barrier, inc=1, device_id=peer, device_id_type=MESH)

    deltas = jnp.maximum(time_step[...], 0.0) + jnp.log1p(jnp.exp(-jnp.abs(time_step[...])))
    delta[...] = deltas
    upto = lax.broadcasted_iota(jnp.int32, (row_count, row_count), 0) <= lax.broadcasted_iota(
        jnp.int32, (row_count, row_count), 1
    )
    head_row = lax.broadcasted_iota(jnp.int32, (head_count, 1), 0)
    rates = jnp.zeros((head_count, 1), jnp.float32)
    for head in range(head_count):
        rates = jnp.where(head_row == head, decay_rate[head], rates)
    running = jnp.dot(
        -rates * deltas, upto.astype(jnp.float32),
        precision=HIGHEST, preferred_element_type=jnp.float32,
    )
    run[...] = running
    tail_heads = jnp.concatenate(
        [running[:, row_count - LANES :], jnp.zeros((LANES - head_count, LANES), jnp.float32)], axis=0
    )
    last_rows = jnp.transpose(tail_heads)[LANES - 8 :, :]
    ends_own[...] = last_rows
    ends[sp] = last_rows

    pl.semaphore_wait(barrier, len(others) + len(siblings))

    started = []

    def go(copy):
        copy.start()
        started.append(copy)

    def remote(source, target, send, recv, peer):
        return pltpu.make_async_remote_copy(
            src_ref=source, dst_ref=target, send_sem=send, recv_sem=recv,
            device_id=peer, device_id_type=MESH,
        )

    after = {"sp": (sp + 1) % sp_count}
    last = slice(row_count - TILE, row_count)
    tails = [
        remote(values.at[last], values_tail, tail_send.at[0], tail_recv.at[0], after),
        remote(keys.at[last], keys_tail, tail_send.at[1], tail_recv.at[1], after),
    ]
    for copy in tails:
        go(copy)

    def both_block(turn):
        peer = flipped(sp, turn, sp_count)
        return remote(
            both_far.at[peer % span], both_got.at[sp], both_send.at[turn - 1], both_recv.at[turn - 1],
            {"sp": peer},
        )

    def down_block(turn):
        peer = flipped(sp, turn, sp_count)
        return remote(
            down_far.at[peer % span], down_got.at[sp], down_send.at[turn - 1], down_recv.at[turn - 1],
            {"sp": peer},
        )

    far_turns = sorted(range(span, sp_count), key=lambda turn: (FAR_ORDER[turn % 4], turn))
    near_turns = list(range(1, span))
    queue = [(both_block, far_turns), (both_block, near_turns), (down_block, far_turns), (down_block, near_turns)]
    queue = [(kind, list(line)) for kind, line in queue]

    def feed(far_count, near_count):
        for first, count in ((0, far_count), (1, near_count)):
            for _ in range(count):
                kind, line = queue[first] if queue[first][1] else queue[first + 2]
                if line:
                    go(kind(line.pop(0)))

    for turn in range(1, sp_count):
        peer = {"sp": flipped(sp, turn, sp_count)}
        go(remote(ends_own, ends.at[sp], ends_send.at[turn - 1], ends_recv.at[turn - 1], peer))
    feed(*FEEDS[0])
    for copy in tails:
        copy.wait_recv()

    def heads_of(g):
        spot = pl.ds(pl.multiple_of(g * GROUP_HEADS, GROUP_HEADS), GROUP_HEADS)
        by_row = run[spot, :]
        return by_row, jnp.transpose(by_row), jnp.transpose(delta[spot, :])

    def value_cols(g):
        return pl.ds(pl.multiple_of(g * group_cols, LANES), group_cols)

    def keys_at(g, first, width):
        return key_rows[g, :, first : first + width]

    kinds = ((0, STATE_WIDE), (2 * STATE_WIDE, STATE_NARROW))

    def state_copy(owner, own_slice, source=None):
        source = place if source is None else source
        return remote(
            state.at[own_slice], state_got.at[source], state_send.at[owner], state_recv.at[source],
            {"sp": base_place + owner},
        )

    def rows_of(owner):
        return pl.ds(pl.multiple_of(owner * slice_rows, 8), slice_rows)

    @pl.loop(0, groups)
    def _(g):
        cols = value_cols(g)
        key_span = pl.ds(pl.multiple_of(g * key_cols, LANES), key_cols)
        first = sp == 0
        before = jnp.where(first, 0.0, values_tail[TILE - 8 :, cols].astype(jnp.float32))
        inner = silu_taps(before, values[:, cols], conv_values[:, cols])
        inputs[:, cols] = inner
        before = jnp.where(first, 0.0, keys_tail[TILE - 8 :, key_span].astype(jnp.float32))
        made = silu_taps(before, keys[:, key_span], conv_keys[:, key_span]).astype(jnp.bfloat16)
        key_rows[g] = made
        by_row, by_col, deltas = heads_of(g)
        states = []
        for kind, (first_col, width) in enumerate(kinds):
            scaled = []
            for head in range(kind * half, (kind + 1) * half):
                own = slice(head * HEAD_SIZE, (head + 1) * HEAD_SIZE)
                to_end = jnp.exp(by_row[head : head + 1, row_count - 1 :] - by_col[:, head : head + 1])
                scaled.append((inner[:, own] * (deltas[:, head : head + 1] * to_end)).astype(jnp.bfloat16))
            states.append(
                lax.dot_general(
                    jnp.concatenate(scaled, axis=1),
                    made[:, first_col : first_col + width],
                    (((0,), (0,)), ((), ())),
                    preferred_element_type=jnp.float32,
                ).astype(jnp.bfloat16)
            )
        base = pl.multiple_of(g * group_rows, 8)
        state[pl.ds(base, wide_rows), :] = states[0]
        fold = STATE_WIDE // STATE_NARROW
        state[pl.ds(base + wide_rows, narrow_rows), :] = jnp.concatenate(
            [states[1][i * narrow_rows : (i + 1) * narrow_rows] for i in range(fold)], axis=1
        )
        per_group = group_rows // slice_rows

        @pl.loop(0, per_group)
        def _(index):
            owner = g * per_group + index

            @pl.when(owner != place)
            def _():
                state_copy(owner, rows_of(owner)).start()

    feed(*FEEDS[1])

    def inside(g):
        cols = value_cols(g)
        by_row, by_col, deltas = heads_of(g)
        inner = inputs[:, cols]
        outs = []
        for kind, (first_col, width) in enumerate(kinds):
            scores = lax.dot_general(
                keys_at(g, first_col + width, width), keys_at(g, first_col, width),
                (((1,), (1,)), ((), ())), preferred_element_type=jnp.float32,
            )
            for head in range(kind * half, (kind + 1) * half):
                own = slice(head * HEAD_SIZE, (head + 1) * HEAD_SIZE)
                gap = causal_rows(by_col[:, head : head + 1] - by_row[head : head + 1, :], row_count)
                mixing = (scores * jnp.exp(gap)).astype(jnp.bfloat16)
                weighted = (inner[:, own] * deltas[:, head : head + 1]).astype(jnp.bfloat16)
                outs.append(
                    jnp.dot(mixing, weighted, preferred_element_type=jnp.float32)
                    + inner[:, own] * skip_gain[g * GROUP_HEADS + head]
                )
        inputs[:, cols] = jnp.concatenate(outs, axis=1)

    ahead = (groups + 1) // 2
    @pl.loop(0, ahead)
    def _(g):
        inside(g)

    for turn in range(1, sp_count):
        peer = {"sp": flipped(sp, turn, sp_count)}
        remote(ends_own, ends.at[sp], ends_send.at[turn - 1], ends_recv.at[turn - 1], peer).wait_recv()

    def span_turn(turn):
        peer = (sp + turn * span) % sp_count
        return remote(
            state_sum, sums_got.at[group_of_spans], total_send.at[turn], total_recv.at[group_of_spans],
            {"sp": peer},
        )

    def carry_all():
        for turn in range(1, span):
            source = flipped(place, turn, span)
            state_copy(place, rows_of(place), source).wait_recv()
        state_got[place] = state[rows_of(place), :]
        first_row = place * slice_rows
        g = first_row // group_rows
        row = lax.broadcasted_iota(jnp.int32, (slice_rows, LANES), 0) + (first_row - g * group_rows)
        lane = lax.broadcasted_iota(jnp.int32, (slice_rows, LANES), 1)
        within = ends[pl.ds(base_place, span), 7, :]
        each = [
            jnp.sum(ends[i * span : (i + 1) * span, 7, :], axis=0, keepdims=True) for i in range(span_count)
        ]
        spans = jnp.concatenate([within] + each, axis=0)
        shift = HEAD_SIZE.bit_length() - 1
        grown = []
        for side in range(STATE_WIDE // STATE_NARROW):
            wide_head = lax.shift_right_logical(row, shift)
            narrow_head = half + side * (narrow_rows // HEAD_SIZE) + lax.shift_right_logical(
                jnp.maximum(row - wide_rows, 0), shift
            )
            head = g * GROUP_HEADS + jnp.where(row < wide_rows, wide_head, narrow_head)
            grown.append(
                jnp.exp(
                    lax.dot_general(
                        (lane == head).astype(jnp.float32), spans, (((1,), (1,)), ((), ())),
                        precision=HIGHEST, preferred_element_type=jnp.float32,
                    )
                )
            )

        def factor(spot):
            return jnp.where(lane < STATE_NARROW, grown[0][:, spot : spot + 1], grown[1][:, spot : spot + 1])

        carry = jnp.zeros((slice_rows, LANES), jnp.float32)
        if span_count > 1:
            for source in range(span):
                carry = carry * factor(source) + state_got[source].astype(jnp.float32)
            state_sum[...] = carry.astype(jnp.bfloat16)
            for turn in range(1, span_count):
                go(span_turn(turn))
            sums_got[group_of_spans] = jnp.zeros((slice_rows, LANES), jnp.bfloat16)
            carry = jnp.zeros((slice_rows, LANES), jnp.float32)
            for turn in range(1, span_count):
                remote(
                    state_sum, sums_got.at[(group_of_spans + turn) % span_count], total_send.at[turn],
                    total_recv.at[(group_of_spans + turn) % span_count], {"sp": (sp + turn * span) % sp_count},
                ).wait_recv()
            for spot in range(span_count - 1):
                further = carry * factor(span + spot) + sums_got[spot].astype(jnp.float32)
                carry = jnp.where(spot < group_of_spans, further, carry)
        for source in range(span):
            states_out[source] = carry.astype(jnp.bfloat16)
            if source + 1 < span:
                carry = carry * factor(source) + state_got[source].astype(jnp.float32)
        states_in[rows_of(place), :] = states_out[place]
        for turn in range(1, span):
            back_copy(place, flipped(place, turn, span)).start()

    def back_copy(owner, target):
        return remote(
            states_out.at[target], states_in.at[rows_of(owner)], back_send.at[target], back_recv.at[owner],
            {"sp": base_place + target},
        )

    carry_all()
    feed(*FEEDS[2])

    @pl.loop(ahead, groups)
    def _(g):
        inside(g)

    gate_copy.wait()
    feed(*FEEDS[3])

    @pl.loop(0, owners)
    def _(owner):
        @pl.when(owner != place)
        def _():
            back_copy(owner, place).wait_recv()

    squares_own[...] = jnp.zeros(squares_own.shape, jnp.float32)

    @pl.loop(0, groups)
    def _(g):
        cols = value_cols(g)
        by_row, by_col, _ = heads_of(g)
        growth = jnp.exp(by_col)
        base = pl.multiple_of(g * group_rows, 8)
        wide_in = states_in[pl.ds(base, wide_rows), :]
        narrow_in = states_in[pl.ds(base + wide_rows, narrow_rows), :]
        reads = [
            lax.dot_general(
                keys_at(g, STATE_WIDE, STATE_WIDE), wide_in,
                (((1,), (1,)), ((), ())), preferred_element_type=jnp.float32,
            )
        ]
        for side in range(STATE_WIDE // STATE_NARROW):
            reads.append(
                lax.dot_general(
                    keys_at(g, 2 * STATE_WIDE + STATE_NARROW, STATE_NARROW),
                    narrow_in[:, side * STATE_NARROW : (side + 1) * STATE_NARROW],
                    (((1,), (1,)), ((), ())), preferred_element_type=jnp.float32,
                )
            )
        read = jnp.concatenate(reads, axis=1)
        parts = [
            read[:, head * HEAD_SIZE : (head + 1) * HEAD_SIZE] * growth[:, head : head + 1]
            for head in range(GROUP_HEADS)
        ]
        gate = gates[:, cols].astype(jnp.float32)
        gated = (inputs[:, cols] + jnp.concatenate(parts, axis=1)) * (gate * jax.nn.sigmoid(gate))
        power = gated * gated
        folded = power[:, :LANES]
        for first in range(LANES, group_cols, LANES):
            folded = folded + power[:, first : first + LANES]
        squares_own[...] += lax.dot_general(
            jnp.ones((8, LANES), jnp.float32), folded, (((1,), (1,)), ((), ())),
            precision=HIGHEST, preferred_element_type=jnp.float32,
        )
        gained[:, cols] = (gated * mix_gain[:, cols]).astype(jnp.bfloat16)

    for step in range(1, tp_count):
        go(remote(squares_own, squares_in.at[step - 1], square_send.at[step - 1], square_recv.at[step - 1], siblings[step - 1]))
    for index, copy in enumerate(weight_copies):
        copy.wait()
        product = jnp.dot(gained[...], slab[index, 0:weight_rows], preferred_element_type=jnp.float32)
        mixed[index * row_count : (index + 1) * row_count, :] = jnp.transpose(product).astype(jnp.bfloat16)
    feed(*FEEDS[4])

    sums = []
    for step in range(1, tp_count):
        peer = pl.ds(pl.multiple_of((tp + step) % tp_count * rows, TILE), rows)
        copy = remote(
            mixed.at[peer], mixed_in.at[step - 1], mix_send.at[step - 1], mix_recv.at[step - 1], siblings[step - 1]
        )
        go(copy)
        sums.append(copy)
    square = squares_own[0:1, :]
    for step in range(1, tp_count):
        remote(squares_own, squares_in.at[step - 1], square_send.at[step - 1], square_recv.at[step - 1], siblings[step - 1]).wait_recv()
        square = square + squares_in[step - 1, 0:1, :]
    inverse = lax.rsqrt(square / (inputs.shape[1] * tp_count) + NORM_FLOOR)
    own_rows = pl.ds(pl.multiple_of(tp * rows, TILE), rows)
    summed = mixed[own_rows, :].astype(jnp.float32)
    for step in range(1, tp_count):
        sums[step - 1].wait_recv()
        summed = summed + mixed_in[step - 1].astype(jnp.float32)
    wide[0, own_rows] = (residual[...].astype(jnp.float32) + summed * inverse).astype(jnp.bfloat16)

    width = both_cols.shape[0]
    quarter = width // 2
    bits = [1 << i for i in range(span.bit_length() - 1)]
    turns = sorted(range(span), key=lambda turn: (turn.bit_count(), turn))
    slot = {turn: i for i, turn in enumerate(turns)}
    orders = [bits[i:] + bits[:i] for i in range(len(bits))]
    parts = row_parts(rows, SHARES[: len(bits)])
    next_span = (sp + span) % sp_count

    def member(turn):
        return {"sp": base_place + flipped(place, turn, span)}

    def sibling(step):
        return siblings[step - 1]

    def part_rows(part):
        size = parts[part].stop - parts[part].start
        return pl.ds(pl.multiple_of(tp * rows + parts[part].start, TILE), size)

    def spread(part, bit, turn):
        place_rows = part_rows(part)
        index = slot[turn ^ bit] - 1
        return pltpu.make_async_remote_copy(
            src_ref=wide.at[slot[turn], place_rows],
            dst_ref=wide.at[slot[turn ^ bit], place_rows],
            send_sem=spread_send.at[part, index],
            recv_sem=spread_recv.at[part, index],
            device_id=member(bit),
            device_id_type=MESH,
        )

    def side(turn, step):
        return pltpu.make_async_remote_copy(
            src_ref=wide.at[slot[turn], own_rows],
            dst_ref=wide.at[slot[turn], own_rows],
            send_sem=side_send.at[slot[turn], step - 1],
            recv_sem=side_recv.at[slot[turn], step - 1],
            device_id=sibling(step),
            device_id_type=MESH,
        )

    def arrived(part, turn):
        order = orders[part]
        last = [bit for bit in order if turn & bit][-1]
        spread(part, last, turn ^ last).wait_recv()

    def onward(part, turn):
        order = orders[part]
        reach = max([-1] + [i for i, bit in enumerate(order) if turn & bit])
        for bit in order[reach + 1 :]:
            go(spread(part, bit, turn))

    for position in range(len(bits)):
        for part in range(len(bits)):
            go(spread(part, orders[part][position], 0))

    def to_sides(turn):
        for step in range(1, tp_count):
            go(side(turn, step))

    def from_sides(turn):
        for step in range(1, tp_count):
            side(turn, step).wait_recv()

    to_sides(0)
    feed(*FEEDS[5])

    def turn_both():
        both_got[sp] = both_far[place]
        for turn in range(1, sp_count):
            both_block(turn).wait_recv()
        chunk = 128
        for first in range(0, features, chunk):
            cols = slice(first, first + chunk)
            each = both_got.shape[1]
            block = both_got[first // each : (first + chunk) // each].reshape(chunk, width)
            block = jnp.transpose(block.astype(jnp.float32))
            both_cols[:, cols] = (block * gain[:, cols]).astype(jnp.bfloat16)

    narrow = down_got.shape[2]
    early = base_place * narrow // rows

    def turn_down(first, waits):
        for turn in waits:
            down_block(turn).wait_recv()
        for index in range(span):
            source = first + index
            block = jnp.transpose(down_got[source].astype(jnp.float32))
            down_rows[pl.ds(pl.multiple_of(source * narrow, narrow), narrow), :] = block.astype(jnp.bfloat16)

    tap_total = taps.shape[1]
    padded = (quarter + LANES - 1) // LANES * LANES
    lines = jnp.concatenate(
        [taps[0].astype(jnp.float32), taps[1].astype(jnp.float32), jnp.zeros((8 - 2 * tap_total, taps.shape[2]), jnp.float32)],
        axis=0,
    )
    hidden_cols = taps.shape[2]
    turned = pltpu.roll(lines, (hidden_cols - place * quarter) % hidden_cols, 1)
    columns = jnp.transpose(turned[:, :padded])
    for tap in range(tap_total):
        for kind in range(2):
            line = columns[:quarter, kind * tap_total + tap : kind * tap_total + tap + 1]
            tap_wide[tap, kind * quarter : (kind + 1) * quarter] = jnp.broadcast_to(line, (quarter, LANES))

    def project(index, turn):
        columns = wide[index]
        squares = jnp.zeros((8, row_count), jnp.float32)
        for first in range(0, features, 256):
            piece = columns[first : first + 256].astype(jnp.float32)
            squares = squares + jnp.sum((piece * piece).reshape(-1, 8, row_count), axis=0)
        mean = jnp.sum(squares, axis=0, keepdims=True) / features
        scale = lax.rsqrt(mean + NORM_FLOOR)
        pre = jnp.dot(both_cols[...], columns, preferred_element_type=jnp.float32) * scale
        both_pre[index] = pre.astype(jnp.bfloat16)
        edges[1 + flipped(place, turn, span)] = pre[:, row_count - LANES :].astype(jnp.bfloat16)

    events = []
    for part in range(len(bits)):
        for turn in turns[1:]:
            order = orders[part]
            key = [i for i, bit in enumerate(order) if turn & bit]
            events.append((max(key), len(key), key, part, turn))
    waiting = {turn: len(bits) for turn in turns[1:]}
    for position, (_, _, _, part, turn) in enumerate(sorted(events)):
        arrived(part, turn)
        onward(part, turn)
        feed(*EVENT_FEEDS.get(position, (0, 0)))
        waiting[turn] -= 1
        if waiting[turn] == 0:
            to_sides(turn)
    feed(2 * sp_count, 2 * sp_count)
    turn_both()
    for turn in turns:
        from_sides(turn)
        project(slot[turn], turn)

    if span < sp_count:
        last = jnp.transpose(edges[span].astype(jnp.float32))
        edge_out[...] = last[LANES - TILE :, :].astype(jnp.bfloat16)
        edge_copy = pltpu.make_async_remote_copy(
            src_ref=edge_out, dst_ref=edge_in, send_sem=edge_send, recv_sem=edge_recv,
            device_id={"sp": next_span}, device_id_type=MESH,
        )
        edge_copy.start()
    edges[0] = jnp.zeros(edges.shape[1:], edges.dtype)

    lane = lax.broadcasted_iota(jnp.int32, (quarter, LANES), 1)

    def taps_of(index, spot):
        for first in range(0, row_count, LANES):
            sums = []
            for kind in range(2):
                own = slice(kind * quarter, (kind + 1) * quarter)
                now = both_pre[index, own, first : first + LANES].astype(jnp.float32)
                if first:
                    past = both_pre[index, own, first - LANES : first].astype(jnp.float32)
                else:
                    past = edges[spot, own, :].astype(jnp.float32)
                tap_count = taps.shape[1]
                summed = tap_wide[tap_count - 1, own, :] * now
                for back in range(1, tap_count):
                    moved = jnp.where(lane < back, pltpu.roll(past, back, 1), pltpu.roll(now, back, 1))
                    summed = summed + tap_wide[tap_count - 1 - back, own, :] * moved
                sums.append(summed)
            value = sums[0] * jax.nn.sigmoid(sums[0]) * sums[1]
            hidden[index, :, first : first + LANES] = value.astype(jnp.bfloat16)

    for turn in turns:
        taps_of(slot[turn], flipped(place, turn, span))
    if span < sp_count:
        edge_copy.wait()
        last = jnp.transpose(edge_in[...].astype(jnp.float32))
        own_edge = jnp.where(base_place == 0, 0.0, last)
        edges[0, :, LANES - TILE :] = own_edge.astype(jnp.bfloat16)
        for turn in turns:
            @pl.when(flipped(place, turn, span) == 0)
            def _():
                taps_of(slot[turn], 0)

    def to_sum(turn, step):
        peer = pl.ds(pl.multiple_of((tp + step) % tp_count * rows, TILE), rows)
        return pltpu.make_async_remote_copy(
            src_ref=slab.at[slot[turn], peer],
            dst_ref=tp_in.at[slot[turn], step - 1],
            send_sem=sum_send.at[slot[turn], step - 1],
            recv_sem=sum_recv.at[slot[turn], step - 1],
            device_id={"tp": (tp + step) % tp_count},
            device_id_type=MESH,
        )

    folds = (fold_a, fold_b, fold_c)

    def fold(part, stage, turn):
        bit = orders[part][stage]
        here = slot[turn ^ bit]
        return pltpu.make_async_remote_copy(
            src_ref=total.at[slot[turn], parts[part]],
            dst_ref=folds[stage].at[here, parts[part]],
            send_sem=fold_send.at[part, slot[turn] - 1],
            recv_sem=fold_recv.at[part, stage, here],
            device_id=member(bit),
            device_id_type=MESH,
        )

    def stage_of(part, turn):
        return min(i for i, bit in enumerate(orders[part]) if turn & bit)

    def multiply(turn, owner):
        step_rows = min(512, rows)
        for first in range(0, rows, step_rows):
            block = pl.ds(pl.multiple_of(owner * rows + first, step_rows), step_rows)
            slab[slot[turn], block] = jnp.dot(
                down_rows[block, :], hidden[slot[turn]], preferred_element_type=jnp.float32
            ).astype(jnp.bfloat16)

        @pl.when(owner != tp)
        def _():
            to_sum(turn, (owner + tp_count - tp) % tp_count).start()

    def add_up(turn):
        summed = slab[slot[turn], own_rows].astype(jnp.float32)
        for step in range(1, tp_count):
            to_sum(turn, step).wait_recv()
            summed = summed + tp_in[slot[turn], step - 1].astype(jnp.float32)
        total[slot[turn]] = summed.astype(jnp.bfloat16)
        if turn:
            for part in range(len(bits)):
                if stage_of(part, turn) == 0:
                    fold(part, 0, turn).start()

    line = turns[::-1]
    down_copy.wait()
    turn_down(base_place, range(1, span))
    for turn in line:
        multiply(turn, early)

    @pl.when(tp == early)
    def _():
        for turn in line:
            add_up(turn)

    for other in range(1, span_count):
        waits = range(span, sp_count) if other == 1 else ()
        turn_down((base_place + other * span) % sp_count, waits)
    for turn in line:
        for other in range(1, tp_count):
            multiply(turn, (early + other) % tp_count)

    @pl.when(tp != early)
    def _():
        for turn in line:
            add_up(turn)

    for stage in range(len(bits)):
        for part in range(len(bits)):
            order = orders[part]
            left = [turn for turn in turns if not any(turn & bit for bit in order[: stage + 1])]
            for turn in sorted(left, key=lambda turn: -turn.bit_count()):
                fold(part, stage, turn ^ order[stage]).wait_recv()
                summed = total[slot[turn], parts[part]].astype(jnp.float32) + folds[stage][
                    slot[turn], parts[part]
                ].astype(jnp.float32)
                if turn:
                    total[slot[turn], parts[part]] = summed.astype(jnp.bfloat16)
                    if stage_of(part, turn) == stage + 1:
                        go(fold(part, stage + 1, turn))
                elif stage + 1 < len(bits):
                    total[0, parts[part]] = summed.astype(jnp.bfloat16)
                else:
                    out[parts[part], :] = (wide[0, part_rows(part)].astype(jnp.float32) + summed).astype(jnp.bfloat16)
    for turn in turns:
        for step in range(1, tp_count):
            to_sum(turn, step).wait_send()
        for part in range(len(bits)):
            if turn and stage_of(part, turn) == 0:
                fold(part, 0, turn).wait_send()
    for copy in started:
        copy.wait_send()


    @pl.loop(0, owners)
    def _(owner):
        @pl.when(owner != place)
        def _():
            state_copy(owner, rows_of(owner)).wait_send()

    for turn in range(1, span):
        back_copy(place, flipped(place, turn, span)).wait_send()


def whole_layer(
    values, keys, gates, time_step, decay_rate, skip_gain, conv_values, conv_keys, mix_gain,
    weight, residual, gate_rows, up_rows, down, gain, taps, span,
):
    sp_count, tp_count = lax.axis_size("sp"), lax.axis_size("tp")
    row_count, inner = values.shape
    rows = residual.shape[0]
    head_count = time_step.shape[0]
    groups = head_count // GROUP_HEADS
    features = weight.shape[1]
    half_rows = GROUP_HEADS // 2 * HEAD_SIZE
    state_rows = groups * (half_rows + half_rows * STATE_NARROW // STATE_WIDE)
    slice_rows = state_rows // span
    quarter = gate_rows.shape[1] // span
    width = 2 * quarter
    both_rows = gate_rows.shape[0]
    levels = span.bit_length() - 1
    bf, f32 = jnp.bfloat16, jnp.float32
    near = pl.BlockSpec(memory_space=pltpu.VMEM)
    small = pl.BlockSpec(memory_space=pltpu.SMEM)
    far = pl.BlockSpec(memory_space=pltpu.MemorySpace.HBM)
    tp_others, others = tp_count - 1, sp_count - 1
    buffers = [
        ((span, both_rows, width), bf),
        ((row_count, inner), bf),
        ((max(span, features // row_count), features, row_count), bf),
        ((TILE, inner), bf),
        ((TILE, keys.shape[1]), bf),
        ((head_count, row_count), f32),
        ((head_count, row_count), f32),
        ((row_count, inner), f32),
        ((groups, row_count, keys.shape[1] // groups), bf),
        ((row_count, inner), bf),
        ((state_rows, LANES), bf),
        ((span, slice_rows, LANES), bf),
        ((span, slice_rows, LANES), bf),
        ((state_rows, LANES), bf),
        ((slice_rows, LANES), bf),
        ((sp_count // span, slice_rows, LANES), bf),
        ((8, LANES), f32),
        ((sp_count, 8, LANES), f32),
        ((8, row_count), f32),
        ((tp_others, 8, row_count), f32),
        ((features, row_count), bf),
        ((tp_others, rows, row_count), bf),
        ((sp_count, both_rows, width), bf),
        ((sp_count,) + down.shape[1:], bf),
        ((span, features, row_count), bf),
        ((width, features), bf),
        ((features, quarter), bf),
        ((span, width, row_count), bf),
        ((span + 1, width, LANES), bf),
        ((TILE, width), bf),
        ((TILE, width), bf),
        ((taps.shape[1], width, LANES), f32),
        ((span, quarter, row_count), bf),
        ((span, tp_others, rows, row_count), bf),
        ((span, rows, row_count), bf),
        ((span, rows, row_count), bf),
        ((4, rows, row_count), bf),
        ((1, rows, row_count), bf),
    ]
    counts = [
        (3,), (features // row_count,), (2,), (2,), (others,), (others,), (span,), (span,),
        (span,), (span,), (sp_count // span,), (sp_count // span,), (tp_others,), (tp_others,), (tp_others,), (tp_others,), (others,), (others,),
        (others,), (others,), (levels, span - 1), (levels, span - 1), (span, tp_others), (span, tp_others), None, None,
        (span, tp_others), (span, tp_others), (levels, span - 1), (levels, levels, span),
    ]
    return pl.pallas_call(
        functools.partial(layer_kernel, sp_count, tp_count, span),
        in_specs=[near, near, far, near, small, small, near, near, near, far, near, near, near, far, near, near],
        out_specs=near,
        out_shape=jax.ShapeDtypeStruct((rows, row_count), bf),
        scratch_shapes=[pltpu.VMEM(shape, dtype) for shape, dtype in buffers]
        + [pltpu.SemaphoreType.DMA(shape) if shape else pltpu.SemaphoreType.DMA for shape in counts],
        compiler_params=pltpu.CompilerParams(
            collective_id=1, has_side_effects=True, vmem_limit_bytes=VMEM_LIMIT
        ),
        cost_estimate=pl.CostEstimate(flops=10**11, bytes_accessed=10**7, transcendentals=10**6),
        name="layer_kernel",
    )(
        values, keys, gates, time_step, decay_rate, skip_gain, conv_values, conv_keys, mix_gain,
        weight, residual, gate_rows, up_rows, down, gain, taps,
    )


def local(
    residual,
    values,
    gate_input,
    group_keys,
    time_step,
    decay_rate,
    skip_gain,
    conv_values,
    conv_keys,
    mix_gain,
    out_weight,
    norm_gain,
    hidden_gate,
    hidden_up,
    hidden_conv,
    hidden_down,
):
    sp_count = lax.axis_size("sp")
    span = min(SPAN, sp_count)
    down = hidden_down.reshape(span, hidden_gate.shape[1] // span, hidden_down.shape[1])
    return whole_layer(
        values, group_keys, gate_input, time_step, decay_rate, skip_gain,
        conv_values, conv_keys, mix_gain[None, :],
        out_weight, residual, hidden_gate, hidden_up, down, norm_gain[None, :], hidden_conv, span,
    )


def solution(mesh):
    in_specs = (
        P("tp", "sp"),
        P("sp", "tp"),
        P("sp", "tp"),
        P("sp", "tp"),
        P("tp", "sp"),
        P("tp"),
        P("tp"),
        P(None, "tp"),
        P(None, "tp"),
        P("tp"),
        P("tp", None),
        P(),
        P("sp", "tp"),
        P("sp", "tp"),
        P(None, None, "tp"),
        P("tp", "sp"),
    )
    out_specs = P("tp", "sp")
    return jax.shard_map(local, mesh=mesh, in_specs=in_specs, out_specs=out_specs, check_vma=False)
```

```python
import functools

import jax
import jax.numpy as jnp
from jax import lax
from jax.experimental import pallas as pl
from jax.experimental.pallas import tpu as pltpu
from jax.sharding import PartitionSpec as P

GROUP_HEADS = 8
HEAD_SIZE = 64
STATE_WIDE = 128
STATE_NARROW = 64

NORM_FLOOR = 0.1
SPAN = 8
EDGE = 8
TILE = 16
FAR_ORDER = (0, 2, 1, 2)
SHARES = (5, 5, 5)
LANES = 128
FEEDS = ((0, 3), (1, 2), (1, 2), (1, 0), (1, 0), (1, 0))
EVENT_FEEDS = {position: (1, 1) for position in range(3, 21)}
VMEM_LIMIT = 63 * 2**20
MESH = pl.DeviceIdType.MESH
HIGHEST = lax.Precision.HIGHEST


def flipped(place, turn, count):
    result = 0
    bit = 1
    while bit < count:
        own = (place // bit) % 2
        result = result + bit * (own + (turn // bit) % 2 * (1 - 2 * own))
        bit *= 2
    return result


def silu_taps(before, rows, taps):
    joined = jnp.concatenate([before.astype(jnp.float32), rows.astype(jnp.float32)], axis=0)
    count = rows.shape[0]
    first = before.shape[0] - taps.shape[0] + 1
    summed = taps[0:1].astype(jnp.float32) * joined[first : first + count]
    for tap in range(1, taps.shape[0]):
        summed = summed + taps[tap : tap + 1].astype(jnp.float32) * joined[
            first + tap : first + tap + count
        ]
    return summed * jax.nn.sigmoid(summed)


def causal_rows(value, count):
    row = lax.broadcasted_iota(jnp.int32, (count, count), 0)
    col = lax.broadcasted_iota(jnp.int32, (count, count), 1)
    return jnp.where(row >= col, value, -jnp.inf)


def row_parts(rows, shares):
    whole = sum(shares)
    bounds = [rows * sum(shares[:part]) // whole // TILE * TILE for part in range(len(shares))] + [rows]
    return [slice(first, last) for first, last in zip(bounds[:-1], bounds[1:])]


def layer_kernel(
    sp_count, tp_count, span,
    values, keys, gates_far, time_step, decay_rate, skip_gain, conv_values, conv_keys, mix_gain,
    weight_far, residual, gate_rows, up_rows, down_far, gain, taps,
    out,
    both_far,
    gates, slab, values_tail, keys_tail, run, delta, inputs, key_rows, gained,
    state, state_got, states_out, states_in, state_sum, sums_got, ends_own, ends, squares_own, squares_in,
    mixed, mixed_in, both_got, down_got,
    wide, both_cols, down_rows, both_pre, edges, edge_out, edge_in, tap_wide, hidden,
    tp_in, total, fold_a, fold_b, fold_c,
    local_sems, weight_sems, tail_send, tail_recv, ends_send, ends_recv, state_send, state_recv,
    back_send, back_recv, total_send, total_recv, square_send, square_recv, mix_send, mix_recv, both_send, both_recv,
    down_send, down_recv, spread_send, spread_recv, side_send, side_recv, edge_send, edge_recv,
    sum_send, sum_recv, fold_send, fold_recv,
):
    sp = lax.axis_index("sp")
    tp = lax.axis_index("tp")
    row_count = values.shape[0]
    head_count = time_step.shape[0]
    groups = head_count // GROUP_HEADS
    half = GROUP_HEADS // 2
    key_cols = 2 * STATE_WIDE + 2 * STATE_NARROW
    group_cols = GROUP_HEADS * HEAD_SIZE
    wide_rows = half * HEAD_SIZE
    narrow_rows = wide_rows * STATE_NARROW // STATE_WIDE
    group_rows = wide_rows + narrow_rows
    slice_rows = states_out.shape[1]
    owners = span
    span_count = sp_count // span
    group_of_spans = sp // span
    rows = residual.shape[0]
    features = wide.shape[1]
    place = sp % span
    base_place = sp - place

    gate_copy = pltpu.make_async_copy(gates_far, gates, local_sems.at[0])
    gate_copy.start()
    weight_rows = weight_far.shape[0]
    weight_copies = []
    for index in range(features // row_count):
        copy = pltpu.make_async_copy(
            weight_far.at[:, index * row_count : (index + 1) * row_count],
            slab.at[index, 0:weight_rows],
            weight_sems.at[index],
        )
        copy.start()
        weight_copies.append(copy)
    down_copy = pltpu.make_async_copy(down_far.at[place], down_got.at[sp], local_sems.at[2])
    down_copy.start()

    quarter = gate_rows.shape[1] // span
    for index in range(span):
        cols = slice(index * quarter, (index + 1) * quarter)
        both_far[index] = jnp.concatenate(
            [gate_rows[:, cols].astype(jnp.float32), up_rows[:, cols].astype(jnp.float32)], axis=1
        ).astype(jnp.bfloat16)

    others = [{"sp": flipped(sp, turn, sp_count)} for turn in range(1, sp_count)]
    siblings = [{"tp": (tp + step) % tp_count} for step in range(1, tp_count)]
    barrier = pltpu.get_barrier_semaphore()
    for peer in others + siblings:
        pl.semaphore_signal(barrier, inc=1, device_id=peer, device_id_type=MESH)

    deltas = jnp.maximum(time_step[...], 0.0) + jnp.log1p(jnp.exp(-jnp.abs(time_step[...])))
    delta[...] = deltas
    upto = lax.broadcasted_iota(jnp.int32, (row_count, row_count), 0) <= lax.broadcasted_iota(
        jnp.int32, (row_count, row_count), 1
    )
    head_row = lax.broadcasted_iota(jnp.int32, (head_count, 1), 0)
    rates = jnp.zeros((head_count, 1), jnp.float32)
    for head in range(head_count):
        rates = jnp.where(head_row == head, decay_rate[head], rates)
    running = jnp.dot(
        -rates * deltas, upto.astype(jnp.float32),
        precision=HIGHEST, preferred_element_type=jnp.float32,
    )
    run[...] = running
    tail_heads = jnp.concatenate(
        [running[:, row_count - LANES :], jnp.zeros((LANES - head_count, LANES), jnp.float32)], axis=0
    )
    last_rows = jnp.transpose(tail_heads)[LANES - 8 :, :]
    ends_own[...] = last_rows
    ends[sp] = last_rows

    pl.semaphore_wait(barrier, len(others) + len(siblings))

    started = []

    def go(copy):
        copy.start()
        started.append(copy)

    def remote(source, target, send, recv, peer):
        return pltpu.make_async_remote_copy(
            src_ref=source, dst_ref=target, send_sem=send, recv_sem=recv,
            device_id=peer, device_id_type=MESH,
        )

    after = {"sp": (sp + 1) % sp_count}
    last = slice(row_count - TILE, row_count)
    tails = [
        remote(values.at[last], values_tail, tail_send.at[0], tail_recv.at[0], after),
        remote(keys.at[last], keys_tail, tail_send.at[1], tail_recv.at[1], after),
    ]
    for copy in tails:
        go(copy)

    def both_block(turn):
        peer = flipped(sp, turn, sp_count)
        return remote(
            both_far.at[peer % span], both_got.at[sp], both_send.at[turn - 1], both_recv.at[turn - 1],
            {"sp": peer},
        )

    def down_block(turn):
        peer = flipped(sp, turn, sp_count)
        return remote(
            down_far.at[peer % span], down_got.at[sp], down_send.at[turn - 1], down_recv.at[turn - 1],
            {"sp": peer},
        )

    far_turns = sorted(range(span, sp_count), key=lambda turn: (FAR_ORDER[turn % 4], turn))
    near_turns = list(range(1, span))
    queue = [(both_block, far_turns), (both_block, near_turns), (down_block, far_turns), (down_block, near_turns)]
    queue = [(kind, list(line)) for kind, line in queue]

    def feed(far_count, near_count):
        for first, count in ((0, far_count), (1, near_count)):
            for _ in range(count):
                kind, line = queue[first] if queue[first][1] else queue[first + 2]
                if line:
                    go(kind(line.pop(0)))

    for turn in range(1, sp_count):
        peer = {"sp": flipped(sp, turn, sp_count)}
        go(remote(ends_own, ends.at[sp], ends_send.at[turn - 1], ends_recv.at[turn - 1], peer))
    feed(*FEEDS[0])
    for copy in tails:
        copy.wait_recv()

    def heads_of(g):
        spot = pl.ds(pl.multiple_of(g * GROUP_HEADS, GROUP_HEADS), GROUP_HEADS)
        by_row = run[spot, :]
        return by_row, jnp.transpose(by_row), jnp.transpose(delta[spot, :])

    def value_cols(g):
        return pl.ds(pl.multiple_of(g * group_cols, LANES), group_cols)

    def keys_at(g, first, width):
        return key_rows[g, :, first : first + width]

    kinds = ((0, STATE_WIDE), (2 * STATE_WIDE, STATE_NARROW))

    def state_copy(owner, own_slice, source=None):
        source = place if source is None else source
        return remote(
            state.at[own_slice], state_got.at[source], state_send.at[owner], state_recv.at[source],
            {"sp": base_place + owner},
        )

    def rows_of(owner):
        return pl.ds(pl.multiple_of(owner * slice_rows, 8), slice_rows)

    @pl.loop(0, groups)
    def _(g):
        cols = value_cols(g)
        key_span = pl.ds(pl.multiple_of(g * key_cols, LANES), key_cols)
        first = sp == 0
        before = jnp.where(first, 0.0, values_tail[TILE - 8 :, cols].astype(jnp.float32))
        inner = silu_taps(before, values[:, cols], conv_values[:, cols])
        inputs[:, cols] = inner
        before = jnp.where(first, 0.0, keys_tail[TILE - 8 :, key_span].astype(jnp.float32))
        made = silu_taps(before, keys[:, key_span], conv_keys[:, key_span]).astype(jnp.bfloat16)
        key_rows[g] = made
        by_row, by_col, deltas = heads_of(g)
        states = []
        for kind, (first_col, width) in enumerate(kinds):
            scaled = []
            for head in range(kind * half, (kind + 1) * half):
                own = slice(head * HEAD_SIZE, (head + 1) * HEAD_SIZE)
                to_end = jnp.exp(by_row[head : head + 1, row_count - 1 :] - by_col[:, head : head + 1])
                scaled.append((inner[:, own] * (deltas[:, head : head + 1] * to_end)).astype(jnp.bfloat16))
            states.append(
                lax.dot_general(
                    jnp.concatenate(scaled, axis=1),
                    made[:, first_col : first_col + width],
                    (((0,), (0,)), ((), ())),
                    preferred_element_type=jnp.float32,
                ).astype(jnp.bfloat16)
            )
        base = pl.multiple_of(g * group_rows, 8)
        state[pl.ds(base, wide_rows), :] = states[0]
        fold = STATE_WIDE // STATE_NARROW
        state[pl.ds(base + wide_rows, narrow_rows), :] = jnp.concatenate(
            [states[1][i * narrow_rows : (i + 1) * narrow_rows] for i in range(fold)], axis=1
        )
        per_group = group_rows // slice_rows

        @pl.loop(0, per_group)
        def _(index):
            owner = g * per_group + index

            @pl.when(owner != place)
            def _():
                state_copy(owner, rows_of(owner)).start()

    feed(*FEEDS[1])

    def inside(g):
        cols = value_cols(g)
        by_row, by_col, deltas = heads_of(g)
        inner = inputs[:, cols]
        outs = []
        for kind, (first_col, width) in enumerate(kinds):
            scores = lax.dot_general(
                keys_at(g, first_col + width, width), keys_at(g, first_col, width),
                (((1,), (1,)), ((), ())), preferred_element_type=jnp.float32,
            )
            for head in range(kind * half, (kind + 1) * half):
                own = slice(head * HEAD_SIZE, (head + 1) * HEAD_SIZE)
                gap = causal_rows(by_col[:, head : head + 1] - by_row[head : head + 1, :], row_count)
                mixing = (scores * jnp.exp(gap)).astype(jnp.bfloat16)
                weighted = (inner[:, own] * deltas[:, head : head + 1]).astype(jnp.bfloat16)
                outs.append(
                    jnp.dot(mixing, weighted, preferred_element_type=jnp.float32)
                    + inner[:, own] * skip_gain[g * GROUP_HEADS + head]
                )
        inputs[:, cols] = jnp.concatenate(outs, axis=1)

    ahead = (groups + 1) // 2
    @pl.loop(0, ahead)
    def _(g):
        inside(g)

    for turn in range(1, sp_count):
        peer = {"sp": flipped(sp, turn, sp_count)}
        remote(ends_own, ends.at[sp], ends_send.at[turn - 1], ends_recv.at[turn - 1], peer).wait_recv()

    def span_turn(turn):
        peer = (sp + turn * span) % sp_count
        return remote(
            state_sum, sums_got.at[group_of_spans], total_send.at[turn], total_recv.at[group_of_spans],
            {"sp": peer},
        )

    def carry_all():
        for turn in range(1, span):
            source = flipped(place, turn, span)
            state_copy(place, rows_of(place), source).wait_recv()
        state_got[place] = state[rows_of(place), :]
        first_row = place * slice_rows
        g = first_row // group_rows
        row = lax.broadcasted_iota(jnp.int32, (slice_rows, LANES), 0) + (first_row - g * group_rows)
        lane = lax.broadcasted_iota(jnp.int32, (slice_rows, LANES), 1)
        within = ends[pl.ds(base_place, span), 7, :]
        each = [
            jnp.sum(ends[i * span : (i + 1) * span, 7, :], axis=0, keepdims=True) for i in range(span_count)
        ]
        spans = jnp.concatenate([within] + each, axis=0)
        shift = HEAD_SIZE.bit_length() - 1
        grown = []
        for side in range(STATE_WIDE // STATE_NARROW):
            wide_head = lax.shift_right_logical(row, shift)
            narrow_head = half + side * (narrow_rows // HEAD_SIZE) + lax.shift_right_logical(
                jnp.maximum(row - wide_rows, 0), shift
            )
            head = g * GROUP_HEADS + jnp.where(row < wide_rows, wide_head, narrow_head)
            grown.append(
                jnp.exp(
                    lax.dot_general(
                        (lane == head).astype(jnp.float32), spans, (((1,), (1,)), ((), ())),
                        precision=HIGHEST, preferred_element_type=jnp.float32,
                    )
                )
            )

        def factor(spot):
            return jnp.where(lane < STATE_NARROW, grown[0][:, spot : spot + 1], grown[1][:, spot : spot + 1])

        carry = jnp.zeros((slice_rows, LANES), jnp.float32)
        if span_count > 1:
            for source in range(span):
                carry = carry * factor(source) + state_got[source].astype(jnp.float32)
            state_sum[...] = carry.astype(jnp.bfloat16)
            for turn in range(1, span_count):
                go(span_turn(turn))
            sums_got[group_of_spans] = jnp.zeros((slice_rows, LANES), jnp.bfloat16)
            carry = jnp.zeros((slice_rows, LANES), jnp.float32)
            for turn in range(1, span_count):
                remote(
                    state_sum, sums_got.at[(group_of_spans + turn) % span_count], total_send.at[turn],
                    total_recv.at[(group_of_spans + turn) % span_count], {"sp": (sp + turn * span) % sp_count},
                ).wait_recv()
            for spot in range(span_count - 1):
                further = carry * factor(span + spot) + sums_got[spot].astype(jnp.float32)
                carry = jnp.where(spot < group_of_spans, further, carry)
        for source in range(span):
            states_out[source] = carry.astype(jnp.bfloat16)
            if source + 1 < span:
                carry = carry * factor(source) + state_got[source].astype(jnp.float32)
        states_in[rows_of(place), :] = states_out[place]
        for turn in range(1, span):
            back_copy(place, flipped(place, turn, span)).start()

    def back_copy(owner, target):
        return remote(
            states_out.at[target], states_in.at[rows_of(owner)], back_send.at[target], back_recv.at[owner],
            {"sp": base_place + target},
        )

    carry_all()
    feed(*FEEDS[2])

    @pl.loop(ahead, groups)
    def _(g):
        inside(g)

    gate_copy.wait()
    feed(*FEEDS[3])

    @pl.loop(0, owners)
    def _(owner):
        @pl.when(owner != place)
        def _():
            back_copy(owner, place).wait_recv()

    squares_own[...] = jnp.zeros(squares_own.shape, jnp.float32)

    @pl.loop(0, groups)
    def _(g):
        cols = value_cols(g)
        by_row, by_col, _ = heads_of(g)
        growth = jnp.exp(by_col)
        base = pl.multiple_of(g * group_rows, 8)
        wide_in = states_in[pl.ds(base, wide_rows), :]
        narrow_in = states_in[pl.ds(base + wide_rows, narrow_rows), :]
        reads = [
            lax.dot_general(
                keys_at(g, STATE_WIDE, STATE_WIDE), wide_in,
                (((1,), (1,)), ((), ())), preferred_element_type=jnp.float32,
            )
        ]
        for side in range(STATE_WIDE // STATE_NARROW):
            reads.append(
                lax.dot_general(
                    keys_at(g, 2 * STATE_WIDE + STATE_NARROW, STATE_NARROW),
                    narrow_in[:, side * STATE_NARROW : (side + 1) * STATE_NARROW],
                    (((1,), (1,)), ((), ())), preferred_element_type=jnp.float32,
                )
            )
        read = jnp.concatenate(reads, axis=1)
        parts = [
            read[:, head * HEAD_SIZE : (head + 1) * HEAD_SIZE] * growth[:, head : head + 1]
            for head in range(GROUP_HEADS)
        ]
        gate = gates[:, cols].astype(jnp.float32)
        gated = (inputs[:, cols] + jnp.concatenate(parts, axis=1)) * (gate * jax.nn.sigmoid(gate))
        power = gated * gated
        folded = power[:, :LANES]
        for first in range(LANES, group_cols, LANES):
            folded = folded + power[:, first : first + LANES]
        squares_own[...] += lax.dot_general(
            jnp.ones((8, LANES), jnp.float32), folded, (((1,), (1,)), ((), ())),
            precision=HIGHEST, preferred_element_type=jnp.float32,
        )
        gained[:, cols] = (gated * mix_gain[:, cols]).astype(jnp.bfloat16)

    for step in range(1, tp_count):
        go(remote(squares_own, squares_in.at[step - 1], square_send.at[step - 1], square_recv.at[step - 1], siblings[step - 1]))
    for index, copy in enumerate(weight_copies):
        copy.wait()
        product = jnp.dot(gained[...], slab[index, 0:weight_rows], preferred_element_type=jnp.float32)
        mixed[index * row_count : (index + 1) * row_count, :] = jnp.transpose(product).astype(jnp.bfloat16)
    feed(*FEEDS[4])

    sums = []
    for step in range(1, tp_count):
        peer = pl.ds(pl.multiple_of((tp + step) % tp_count * rows, TILE), rows)
        copy = remote(
            mixed.at[peer], mixed_in.at[step - 1], mix_send.at[step - 1], mix_recv.at[step - 1], siblings[step - 1]
        )
        go(copy)
        sums.append(copy)
    square = squares_own[0:1, :]
    for step in range(1, tp_count):
        remote(squares_own, squares_in.at[step - 1], square_send.at[step - 1], square_recv.at[step - 1], siblings[step - 1]).wait_recv()
        square = square + squares_in[step - 1, 0:1, :]
    inverse = lax.rsqrt(square / (inputs.shape[1] * tp_count) + NORM_FLOOR)
    own_rows = pl.ds(pl.multiple_of(tp * rows, TILE), rows)
    summed = mixed[own_rows, :].astype(jnp.float32)
    for step in range(1, tp_count):
        sums[step - 1].wait_recv()
        summed = summed + mixed_in[step - 1].astype(jnp.float32)
    wide[0, own_rows] = (residual[...].astype(jnp.float32) + summed * inverse).astype(jnp.bfloat16)

    width = both_cols.shape[0]
    quarter = width // 2
    bits = [1 << i for i in range(span.bit_length() - 1)]
    turns = sorted(range(span), key=lambda turn: (turn.bit_count(), turn))
    slot = {turn: i for i, turn in enumerate(turns)}
    orders = [bits[i:] + bits[:i] for i in range(len(bits))]
    parts = row_parts(rows, SHARES[: len(bits)])
    next_span = (sp + span) % sp_count

    def member(turn):
        return {"sp": base_place + flipped(place, turn, span)}

    def sibling(step):
        return siblings[step - 1]

    def part_rows(part):
        size = parts[part].stop - parts[part].start
        return pl.ds(pl.multiple_of(tp * rows + parts[part].start, TILE), size)

    def spread(part, bit, turn):
        place_rows = part_rows(part)
        index = slot[turn ^ bit] - 1
        return pltpu.make_async_remote_copy(
            src_ref=wide.at[slot[turn], place_rows],
            dst_ref=wide.at[slot[turn ^ bit], place_rows],
            send_sem=spread_send.at[part, index],
            recv_sem=spread_recv.at[part, index],
            device_id=member(bit),
            device_id_type=MESH,
        )

    def side(turn, step):
        return pltpu.make_async_remote_copy(
            src_ref=wide.at[slot[turn], own_rows],
            dst_ref=wide.at[slot[turn], own_rows],
            send_sem=side_send.at[slot[turn], step - 1],
            recv_sem=side_recv.at[slot[turn], step - 1],
            device_id=sibling(step),
            device_id_type=MESH,
        )

    def arrived(part, turn):
        order = orders[part]
        last = [bit for bit in order if turn & bit][-1]
        spread(part, last, turn ^ last).wait_recv()

    def onward(part, turn):
        order = orders[part]
        reach = max([-1] + [i for i, bit in enumerate(order) if turn & bit])
        for bit in order[reach + 1 :]:
            go(spread(part, bit, turn))

    for position in range(len(bits)):
        for part in range(len(bits)):
            go(spread(part, orders[part][position], 0))

    def to_sides(turn):
        for step in range(1, tp_count):
            go(side(turn, step))

    def from_sides(turn):
        for step in range(1, tp_count):
            side(turn, step).wait_recv()

    to_sides(0)
    feed(*FEEDS[5])

    def turn_both():
        both_got[sp] = both_far[place]
        for turn in range(1, sp_count):
            both_block(turn).wait_recv()
        chunk = 128
        for first in range(0, features, chunk):
            cols = slice(first, first + chunk)
            each = both_got.shape[1]
            block = both_got[first // each : (first + chunk) // each].reshape(chunk, width)
            block = jnp.transpose(block.astype(jnp.float32))
            both_cols[:, cols] = (block * gain[:, cols]).astype(jnp.bfloat16)

    narrow = down_got.shape[2]
    early = base_place * narrow // rows

    def turn_down(first, waits):
        for turn in waits:
            down_block(turn).wait_recv()
        for index in range(span):
            source = first + index
            block = jnp.transpose(down_got[source].astype(jnp.float32))
            down_rows[pl.ds(pl.multiple_of(source * narrow, narrow), narrow), :] = block.astype(jnp.bfloat16)

    tap_total = taps.shape[1]
    padded = (quarter + LANES - 1) // LANES * LANES
    lines = jnp.concatenate(
        [taps[0].astype(jnp.float32), taps[1].astype(jnp.float32), jnp.zeros((8 - 2 * tap_total, taps.shape[2]), jnp.float32)],
        axis=0,
    )
    hidden_cols = taps.shape[2]
    turned = pltpu.roll(lines, (hidden_cols - place * quarter) % hidden_cols, 1)
    columns = jnp.transpose(turned[:, :padded])
    for tap in range(tap_total):
        for kind in range(2):
            line = columns[:quarter, kind * tap_total + tap : kind * tap_total + tap + 1]
            tap_wide[tap, kind * quarter : (kind + 1) * quarter] = jnp.broadcast_to(line, (quarter, LANES))

    def project(index, turn):
        columns = wide[index]
        squares = jnp.zeros((8, row_count), jnp.float32)
        for first in range(0, features, 256):
            piece = columns[first : first + 256].astype(jnp.float32)
            squares = squares + jnp.sum((piece * piece).reshape(-1, 8, row_count), axis=0)
        mean = jnp.sum(squares, axis=0, keepdims=True) / features
        scale = lax.rsqrt(mean + NORM_FLOOR)
        pre = jnp.dot(both_cols[...], columns, preferred_element_type=jnp.float32) * scale
        both_pre[index] = pre.astype(jnp.bfloat16)
        edges[1 + flipped(place, turn, span)] = pre[:, row_count - LANES :].astype(jnp.bfloat16)

    events = []
    for part in range(len(bits)):
        for turn in turns[1:]:
            order = orders[part]
            key = [i for i, bit in enumerate(order) if turn & bit]
            events.append((max(key), len(key), key, part, turn))
    waiting = {turn: len(bits) for turn in turns[1:]}
    for position, (_, _, _, part, turn) in enumerate(sorted(events)):
        arrived(part, turn)
        onward(part, turn)
        feed(*EVENT_FEEDS.get(position, (0, 0)))
        waiting[turn] -= 1
        if waiting[turn] == 0:
            to_sides(turn)
    feed(2 * sp_count, 2 * sp_count)
    turn_both()
    for turn in turns:
        from_sides(turn)
        project(slot[turn], turn)

    if span < sp_count:
        last = jnp.transpose(edges[span].astype(jnp.float32))
        edge_out[...] = last[LANES - TILE :, :].astype(jnp.bfloat16)
        edge_copy = pltpu.make_async_remote_copy(
            src_ref=edge_out, dst_ref=edge_in, send_sem=edge_send, recv_sem=edge_recv,
            device_id={"sp": next_span}, device_id_type=MESH,
        )
        edge_copy.start()
    edges[0] = jnp.zeros(edges.shape[1:], edges.dtype)

    lane = lax.broadcasted_iota(jnp.int32, (quarter, LANES), 1)

    def taps_of(index, spot):
        for first in range(0, row_count, LANES):
            sums = []
            for kind in range(2):
                own = slice(kind * quarter, (kind + 1) * quarter)
                now = both_pre[index, own, first : first + LANES].astype(jnp.float32)
                if first:
                    past = both_pre[index, own, first - LANES : first].astype(jnp.float32)
                else:
                    past = edges[spot, own, :].astype(jnp.float32)
                tap_count = taps.shape[1]
                summed = tap_wide[tap_count - 1, own, :] * now
                for back in range(1, tap_count):
                    moved = jnp.where(lane < back, pltpu.roll(past, back, 1), pltpu.roll(now, back, 1))
                    summed = summed + tap_wide[tap_count - 1 - back, own, :] * moved
                sums.append(summed)
            value = sums[0] * jax.nn.sigmoid(sums[0]) * sums[1]
            hidden[index, :, first : first + LANES] = value.astype(jnp.bfloat16)

    for turn in turns:
        taps_of(slot[turn], flipped(place, turn, span))
    if span < sp_count:
        edge_copy.wait()
        last = jnp.transpose(edge_in[...].astype(jnp.float32))
        own_edge = jnp.where(base_place == 0, 0.0, last)
        edges[0, :, LANES - TILE :] = own_edge.astype(jnp.bfloat16)
        for turn in turns:
            @pl.when(flipped(place, turn, span) == 0)
            def _():
                taps_of(slot[turn], 0)

    def to_sum(turn, step):
        peer = pl.ds(pl.multiple_of((tp + step) % tp_count * rows, TILE), rows)
        return pltpu.make_async_remote_copy(
            src_ref=slab.at[slot[turn], peer],
            dst_ref=tp_in.at[slot[turn], step - 1],
            send_sem=sum_send.at[slot[turn], step - 1],
            recv_sem=sum_recv.at[slot[turn], step - 1],
            device_id={"tp": (tp + step) % tp_count},
            device_id_type=MESH,
        )

    folds = (fold_a, fold_b, fold_c)

    def fold(part, stage, turn):
        bit = orders[part][stage]
        here = slot[turn ^ bit]
        return pltpu.make_async_remote_copy(
            src_ref=total.at[slot[turn], parts[part]],
            dst_ref=folds[stage].at[here, parts[part]],
            send_sem=fold_send.at[part, slot[turn] - 1],
            recv_sem=fold_recv.at[part, stage, here],
            device_id=member(bit),
            device_id_type=MESH,
        )

    def stage_of(part, turn):
        return min(i for i, bit in enumerate(orders[part]) if turn & bit)

    def multiply(turn, owner):
        step_rows = min(512, rows)
        for first in range(0, rows, step_rows):
            block = pl.ds(pl.multiple_of(owner * rows + first, step_rows), step_rows)
            slab[slot[turn], block] = jnp.dot(
                down_rows[block, :], hidden[slot[turn]], preferred_element_type=jnp.float32
            ).astype(jnp.bfloat16)

        @pl.when(owner != tp)
        def _():
            to_sum(turn, (owner + tp_count - tp) % tp_count).start()

    def add_up(turn):
        summed = slab[slot[turn], own_rows].astype(jnp.float32)
        for step in range(1, tp_count):
            to_sum(turn, step).wait_recv()
            summed = summed + tp_in[slot[turn], step - 1].astype(jnp.float32)
        total[slot[turn]] = summed.astype(jnp.bfloat16)
        if turn:
            for part in range(len(bits)):
                if stage_of(part, turn) == 0:
                    fold(part, 0, turn).start()

    line = turns[::-1]
    down_copy.wait()
    turn_down(base_place, range(1, span))
    def pipelined(chosen, owners_of):
        for position, turn in enumerate(line + [None]):
            if turn is not None:
                for owner in owners_of:
                    multiply(turn, owner)
            if position:
                pl.when(chosen)(functools.partial(add_up, line[position - 1]))

    pipelined(tp == early, [early])

    for other in range(1, span_count):
        waits = range(span, sp_count) if other == 1 else ()
        turn_down((base_place + other * span) % sp_count, waits)
    pipelined(tp != early, [(early + other) % tp_count for other in range(1, tp_count)])

    for stage in range(len(bits)):
        for part in range(len(bits)):
            order = orders[part]
            left = [turn for turn in turns if not any(turn & bit for bit in order[: stage + 1])]
            for turn in sorted(left, key=lambda turn: -turn.bit_count()):
                fold(part, stage, turn ^ order[stage]).wait_recv()
                summed = total[slot[turn], parts[part]].astype(jnp.float32) + folds[stage][
                    slot[turn], parts[part]
                ].astype(jnp.float32)
                if turn:
                    total[slot[turn], parts[part]] = summed.astype(jnp.bfloat16)
                    if stage_of(part, turn) == stage + 1:
                        go(fold(part, stage + 1, turn))
                elif stage + 1 < len(bits):
                    total[0, parts[part]] = summed.astype(jnp.bfloat16)
                else:
                    out[parts[part], :] = (wide[0, part_rows(part)].astype(jnp.float32) + summed).astype(jnp.bfloat16)
    for turn in turns:
        for step in range(1, tp_count):
            to_sum(turn, step).wait_send()
        for part in range(len(bits)):
            if turn and stage_of(part, turn) == 0:
                fold(part, 0, turn).wait_send()
    for copy in started:
        copy.wait_send()


    @pl.loop(0, owners)
    def _(owner):
        @pl.when(owner != place)
        def _():
            state_copy(owner, rows_of(owner)).wait_send()

    for turn in range(1, span):
        back_copy(place, flipped(place, turn, span)).wait_send()


def whole_layer(
    values, keys, gates, time_step, decay_rate, skip_gain, conv_values, conv_keys, mix_gain,
    weight, residual, gate_rows, up_rows, down, gain, taps, span,
):
    sp_count, tp_count = lax.axis_size("sp"), lax.axis_size("tp")
    row_count, inner = values.shape
    rows = residual.shape[0]
    head_count = time_step.shape[0]
    groups = head_count // GROUP_HEADS
    features = weight.shape[1]
    half_rows = GROUP_HEADS // 2 * HEAD_SIZE
    state_rows = groups * (half_rows + half_rows * STATE_NARROW // STATE_WIDE)
    slice_rows = state_rows // span
    quarter = gate_rows.shape[1] // span
    width = 2 * quarter
    both_rows = gate_rows.shape[0]
    levels = span.bit_length() - 1
    bf, f32 = jnp.bfloat16, jnp.float32
    near = pl.BlockSpec(memory_space=pltpu.VMEM)
    small = pl.BlockSpec(memory_space=pltpu.SMEM)
    far = pl.BlockSpec(memory_space=pltpu.MemorySpace.HBM)
    tp_others, others = tp_count - 1, sp_count - 1
    buffers = [
        ((span, both_rows, width), bf),
        ((row_count, inner), bf),
        ((max(span, features // row_count), features, row_count), bf),
        ((TILE, inner), bf),
        ((TILE, keys.shape[1]), bf),
        ((head_count, row_count), f32),
        ((head_count, row_count), f32),
        ((row_count, inner), f32),
        ((groups, row_count, keys.shape[1] // groups), bf),
        ((row_count, inner), bf),
        ((state_rows, LANES), bf),
        ((span, slice_rows, LANES), bf),
        ((span, slice_rows, LANES), bf),
        ((state_rows, LANES), bf),
        ((slice_rows, LANES), bf),
        ((sp_count // span, slice_rows, LANES), bf),
        ((8, LANES), f32),
        ((sp_count, 8, LANES), f32),
        ((8, row_count), f32),
        ((tp_others, 8, row_count), f32),
        ((features, row_count), bf),
        ((tp_others, rows, row_count), bf),
        ((sp_count, both_rows, width), bf),
        ((sp_count,) + down.shape[1:], bf),
        ((span, features, row_count), bf),
        ((width, features), bf),
        ((features, quarter), bf),
        ((span, width, row_count), bf),
        ((span + 1, width, LANES), bf),
        ((TILE, width), bf),
        ((TILE, width), bf),
        ((taps.shape[1], width, LANES), f32),
        ((span, quarter, row_count), bf),
        ((span, tp_others, rows, row_count), bf),
        ((span, rows, row_count), bf),
        ((span, rows, row_count), bf),
        ((4, rows, row_count), bf),
        ((1, rows, row_count), bf),
    ]
    counts = [
        (3,), (features // row_count,), (2,), (2,), (others,), (others,), (span,), (span,),
        (span,), (span,), (sp_count // span,), (sp_count // span,), (tp_others,), (tp_others,), (tp_others,), (tp_others,), (others,), (others,),
        (others,), (others,), (levels, span - 1), (levels, span - 1), (span, tp_others), (span, tp_others), None, None,
        (span, tp_others), (span, tp_others), (levels, span - 1), (levels, levels, span),
    ]
    return pl.pallas_call(
        functools.partial(layer_kernel, sp_count, tp_count, span),
        in_specs=[near, near, far, near, small, small, near, near, near, far, near, near, near, far, near, near],
        out_specs=near,
        out_shape=jax.ShapeDtypeStruct((rows, row_count), bf),
        scratch_shapes=[pltpu.VMEM(shape, dtype) for shape, dtype in buffers]
        + [pltpu.SemaphoreType.DMA(shape) if shape else pltpu.SemaphoreType.DMA for shape in counts],
        compiler_params=pltpu.CompilerParams(
            collective_id=1, has_side_effects=True, vmem_limit_bytes=VMEM_LIMIT
        ),
        cost_estimate=pl.CostEstimate(flops=10**11, bytes_accessed=10**7, transcendentals=10**6),
        name="layer_kernel",
    )(
        values, keys, gates, time_step, decay_rate, skip_gain, conv_values, conv_keys, mix_gain,
        weight, residual, gate_rows, up_rows, down, gain, taps,
    )


def local(
    residual,
    values,
    gate_input,
    group_keys,
    time_step,
    decay_rate,
    skip_gain,
    conv_values,
    conv_keys,
    mix_gain,
    out_weight,
    norm_gain,
    hidden_gate,
    hidden_up,
    hidden_conv,
    hidden_down,
):
    sp_count = lax.axis_size("sp")
    span = min(SPAN, sp_count)
    down = hidden_down.reshape(span, hidden_gate.shape[1] // span, hidden_down.shape[1])
    return whole_layer(
        values, group_keys, gate_input, time_step, decay_rate, skip_gain,
        conv_values, conv_keys, mix_gain[None, :],
        out_weight, residual, hidden_gate, hidden_up, down, norm_gain[None, :], hidden_conv, span,
    )


def solution(mesh):
    in_specs = (
        P("tp", "sp"),
        P("sp", "tp"),
        P("sp", "tp"),
        P("sp", "tp"),
        P("tp", "sp"),
        P("tp"),
        P("tp"),
        P(None, "tp"),
        P(None, "tp"),
        P("tp"),
        P("tp", None),
        P(),
        P("sp", "tp"),
        P("sp", "tp"),
        P(None, None, "tp"),
        P("tp", "sp"),
    )
    out_specs = P("tp", "sp")
    return jax.shard_map(local, mesh=mesh, in_specs=in_specs, out_specs=out_specs, check_vma=False)
```
